32 devices in a mesh: sp: 4 (over z), fs: 4 (over y, x), tp: 2 (over core).
Axes of the slice: x: 2, y: 2, z: 4, core: 2. Of those that a mesh axis runs over, the one named last changes fastest.
Arguments:
- tokens: bfloat16 [4, 1024, 2048], P('fs', 'sp', 'tp'), may hold values from -6 to 6
- norm_gain: float32 [2048], replicated, may hold values from 0.1 to 1.9
- w_query: bfloat16 [2048, 1024], P(('sp', 'fs'), 'tp'), may hold values from -0.125 to 0.125
- forget_weight: bfloat16 [2048, 1024], P(('sp', 'fs'), 'tp'), may hold values from -0.125 to 0.125
- w_input: bfloat16 [2048, 1024], P(('sp', 'fs'), 'tp'), may hold values from -8 to 8
- w_outgate: bfloat16 [2048, 1024], P(('sp', 'fs'), 'tp'), may hold values from -0.125 to 0.125
- w_pool: bfloat16 [2048, 1024], P(('sp', 'fs'), 'tp'), may hold values from -0.125 to 0.125
- forget_gap: float32 [1024], P('tp'), may hold values from 0 to 0.07
- extra_decay: float32 [4, 1024, 8], P('fs', 'sp', 'tp'), may hold values from -0.61 to 0
- rec_gain: float32 [1024], P('tp'), may hold values from 0.1 to 1.9
- group_weight: bfloat16 [4, 256, 256], replicated, may hold values from -0.375 to 0.375
- pool_gain: float32 [1024], P('tp'), may hold values from 0.1 to 1.9
- recurrent_output_weight: bfloat16 [1024, 2048], P('tp', ('sp', 'fs')), may hold values from -0.1875 to 0.1875
- w_out_pool: bfloat16 [1024, 2048], P('tp', ('sp', 'fs')), may hold values from -0.1875 to 0.1875
Outputs:
- mixed_out: bfloat16 [4, 1024, 2048], P('fs', ('sp', 'tp'))
The draws below stay inside these ranges and needn't reach their ends.
All inputs are finite; a program needn't handle non-finite values.
Results may differ from the reference program's by a relative error of at most 0.011.
Values may be sent and summed in bfloat16 or wider, within the bound.
A program may use at most 64 MiB of HBM per device.

```python
import math
import jax
import jax.numpy as jnp
from jax import lax

D = 2048
HGRN_HEADS = 8
HEAD_DIM = 128
D_HGRN = 1024
D_POOL = 1024
POOL_GROUPS = 4
GROUP_DIM = 256
BLOCK = 64
TOK_DEV = 256
SEQ_LEN = 1024
SEQS = 4
N_TP = 2


def head_speeds(key):
    order = jax.random.permutation(jax.random.fold_in(key, 17), HGRN_HEADS)
    fast_count = HGRN_HEADS // 2
    return order < fast_count


def draw_forget_gap(key, part):
    fast_heads = head_speeds(key)
    spread = jax.random.uniform(jax.random.fold_in(key, 5), (HGRN_HEADS, HEAD_DIM), jnp.float32)
    fast_gap = 0.025 * jnp.exp(spread * math.log(2.8))
    slow_gap = 0.3 * jnp.exp(spread * math.log(4.0)) / SEQ_LEN
    return jnp.where(fast_heads[:, None], fast_gap, slow_gap).reshape(D_HGRN).astype(jnp.float32)


def draw_w_input(key, part):
    fast_heads = head_speeds(key)
    normal_draw = jnp.clip(jax.random.normal(jax.random.fold_in(key, 3), (D, D_HGRN), jnp.float32), -6.0, 6.0)
    slow_scale = math.sqrt(SEQ_LEN) / 4.0
    column_scale = jnp.repeat(jnp.where(fast_heads, 1.0, slow_scale), HEAD_DIM)
    return (normal_draw * column_scale[None, :] / math.sqrt(D)).astype(jnp.bfloat16)


def draw_extra_decay(key, part):
    base_key = jax.random.fold_in(key, 9)
    rate_key, spot_key, depth_key = jax.random.split(base_key, 3)
    block_total = SEQ_LEN // TOK_DEV
    level = jax.random.uniform(rate_key, (SEQS, block_total, 1, HGRN_HEADS), jnp.float32)
    shrink_factor_list = 0.15 * jnp.exp(level * math.log(4.0)) / SEQ_LEN
    shrink_factor_list = jnp.broadcast_to(shrink_factor_list, (SEQS, block_total, TOK_DEV, HGRN_HEADS)).reshape(SEQS, SEQ_LEN, HGRN_HEADS)
    first_spot = jax.random.randint(jax.random.fold_in(spot_key, 1), (SEQS, 1, HGRN_HEADS, 1), 0, SEQ_LEN)
    spot_offset = jax.random.randint(jax.random.fold_in(spot_key, 2), (SEQS, 1, HGRN_HEADS, 1), 1, SEQ_LEN)
    second_spot = (first_spot + spot_offset) % SEQ_LEN
    probe_locations = jnp.concatenate([first_spot, second_spot], axis=3)
    layer_tiers = jnp.log(0.55 + 0.25 * jax.random.uniform(depth_key, (SEQS, 1, HGRN_HEADS, 2), jnp.float32))
    symbol_indices = jnp.arange(SEQ_LEN, dtype=jnp.int32)[None, :, None, None]
    spike_clusters = jnp.sum(jnp.where(symbol_indices == probe_locations, layer_tiers, 0.0), axis=3)
    return (spike_clusters - shrink_factor_list).astype(jnp.float32)


def level_of(key, dims, cuts, smallest, largest):
    gain = 1.0
    for axis_at, shards_of in cuts:
        draws = jax.random.uniform(jax.random.fold_in(jax.random.fold_in(key, 6), axis_at), (shards_of,), jnp.float32, smallest / len(cuts), largest / len(cuts))
        gain = gain * jnp.repeat(jnp.exp(draws), dims[axis_at] // shards_of).reshape((-1,) + (1,) * (len(dims) - 1 - axis_at))
    return gain


def noise(key, extent, scale, bound, cuts=(), held_as=jnp.bfloat16):
    drawn = jax.random.normal(key, extent, jnp.float32) * scale
    if len(cuts) > 0:
        drawn = level_of(key, extent, cuts, -0.22, 0.18) * drawn
    return jnp.clip(drawn, min=-bound, max=bound).astype(held_as)


def setup_inputs(seed: int = 0) -> dict:
    key_list = jax.random.split(jax.random.key(seed), 15)
    return {
        "tokens": noise(key_list[0], (SEQS, SEQ_LEN, D), 1.0, 6.0, ((0, 4), (1, 4), (2, 2))),
        "norm_gain": jnp.clip(1.0 + 0.18 * jax.random.normal(key_list[1], (D,), jnp.float32), 0.1, 1.9),
        "w_query": noise(key_list[2], (D, D_HGRN), D ** -0.5, 0.125, ((0, 16), (1, 2))),
        "forget_weight": noise(key_list[3], (D, D_HGRN), D ** -0.5, 0.125, ((0, 16), (1, 2))),
        "w_input": draw_w_input(jax.random.fold_in(key_list[14], 71), 0),
        "w_outgate": noise(key_list[5], (D, D_HGRN), D ** -0.5, 0.125, ((0, 16), (1, 2))),
        "w_pool": noise(key_list[6], (D, D_POOL), D ** -0.5, 0.125, ((0, 16), (1, 2))),
        "forget_gap": draw_forget_gap(jax.random.fold_in(key_list[14], 71), 0),
        "extra_decay": draw_extra_decay(jax.random.fold_in(key_list[14], 71), 0),
        "rec_gain": jnp.clip(1.0 + 0.18 * jax.random.normal(key_list[9], (D_HGRN,), jnp.float32), 0.1, 1.9),
        "group_weight": noise(key_list[10], (POOL_GROUPS, GROUP_DIM, GROUP_DIM), GROUP_DIM ** -0.5, 0.375),
        "pool_gain": jnp.clip(1.0 + 0.18 * jax.random.normal(key_list[11], (D_POOL,), jnp.float32), 0.1, 1.9),
        "recurrent_output_weight": noise(key_list[12], (D_HGRN, D), D_HGRN ** -0.5, 0.1875, ((0, 2), (1, 16))),
        "w_out_pool": noise(key_list[13], (D_POOL, D), D_POOL ** -0.5, 0.1875, ((0, 2), (1, 16))),
    }


EPS = 1e-06
HIGH = lax.Precision.HIGHEST

def recurrence(queries, input_gate, values, log_forget):
    block_count = queries.shape[0] // BLOCK
    shaped = tuple((arr.reshape(block_count, BLOCK, HGRN_HEADS, HEAD_DIM) for arr in (queries, input_gate, values, log_forget)))
    causal = jnp.tril(jnp.ones((BLOCK, BLOCK), jnp.bool_))

    def advance(carried, pieces):
        q_blk, k_blk, v_blk, g_blk = pieces
        within = jnp.cumsum(g_blk, axis=0)
        block_end = within[-1]
        q_up = q_blk * jnp.exp(within)
        scores = jnp.einsum('thd,shd->hts', q_up, k_blk * jnp.exp(-within), precision=HIGH)
        scores = jnp.where(causal, scores, 0.0)
        result = jnp.einsum('hts,she->the', scores, v_blk, precision=HIGH)
        result = result + jnp.einsum('thd,hde->the', q_up, carried, precision=HIGH)
        fresh_input = jnp.einsum('shd,she->hde', k_blk * jnp.exp(block_end[None] - within), v_blk, precision=HIGH)
        carried = jnp.exp(block_end)[:, :, None] * carried + fresh_input
        return (carried, result)
    initial = jnp.zeros((HGRN_HEADS, HEAD_DIM, HEAD_DIM), jnp.float32)
    _, results = lax.scan(advance, initial, shaped)
    return results.reshape(queries.shape[0], D_HGRN)

def pooling(z_pool, group_weight, pool_gain):
    seq_rows = z_pool.shape[0]
    reach_rows = 2 ** POOL_GROUPS
    values = z_pool.astype(jnp.float32)
    padded = jnp.pad(values, ((reach_rows, 0), (0, 0)))
    symbol_indices = jnp.arange(seq_rows, dtype=jnp.int32)
    outputs = []
    for group_idx in range(POOL_GROUPS):
        window_len = 2 ** (group_idx + 1)
        lowest_column_index = group_idx * GROUP_DIM
        high_col = lowest_column_index + GROUP_DIM
        window = padded[reach_rows:reach_rows + seq_rows, lowest_column_index:high_col]
        for shift_idx in range(1, window_len):
            window = window + padded[reach_rows - shift_idx:reach_rows - shift_idx + seq_rows, lowest_column_index:high_col]
        counts_here = jnp.minimum(symbol_indices + 1, window_len).astype(jnp.float32)[:, None]
        pooled = (window / counts_here - values[:, lowest_column_index:high_col]).astype(jnp.bfloat16)
        mapped = jnp.dot(pooled, group_weight[group_idx], preferred_element_type=jnp.float32)
        outputs.append((mapped * pool_gain[lowest_column_index:high_col]).astype(jnp.bfloat16))
    return jnp.concatenate(outputs, axis=1)

def one_sequence(tokens_seq, extra_seq, weights):
    norm_gain, w_query, forget_weight, w_input, w_outgate, w_pool, forget_gap, rec_gain, group_weight, pool_gain, recurrent_output_weight, w_out_pool = weights
    features_f = tokens_seq.astype(jnp.float32)
    token_scale = lax.rsqrt(lax.optimization_barrier(jnp.mean(features_f * features_f, axis=-1, keepdims=True)) + EPS)
    normed = (features_f * token_scale * norm_gain).astype(jnp.bfloat16)

    def project(matrix):
        return jnp.dot(normed, matrix, preferred_element_type=jnp.float32).astype(jnp.bfloat16)
    z_query = project(w_query)
    z_forget = project(forget_weight)
    z_input = project(w_input)
    z_outgate = project(w_outgate)
    z_pool = project(w_pool)
    input_gate = forget_gap * jax.nn.sigmoid(-z_forget.astype(jnp.float32))
    log_forget = jnp.log1p(-input_gate) + jnp.repeat(extra_seq, HEAD_DIM, axis=1)
    queries = jax.nn.silu(z_query.astype(jnp.float32))
    recurrent = recurrence(queries, input_gate, z_input.astype(jnp.float32), log_forget)
    rec_scale = lax.rsqrt(lax.optimization_barrier(jnp.mean(recurrent * recurrent, axis=-1, keepdims=True)) + EPS)
    recurrent_output = (recurrent * rec_scale * rec_gain * jax.nn.silu(z_outgate.astype(jnp.float32))).astype(jnp.bfloat16)
    pool_out = pooling(z_pool, group_weight, pool_gain)
    rec_rows = D_HGRN // N_TP
    pool_rows = D_POOL // N_TP
    summed_out = jnp.zeros((tokens_seq.shape[0], D), jnp.float32)
    for block_idx in range(N_TP):
        rec_lo = block_idx * rec_rows
        pool_lo = block_idx * pool_rows
        partial_sum = jnp.dot(recurrent_output[:, rec_lo:rec_lo + rec_rows], recurrent_output_weight[rec_lo:rec_lo + rec_rows], preferred_element_type=jnp.float32) + jnp.dot(pool_out[:, pool_lo:pool_lo + pool_rows], w_out_pool[pool_lo:pool_lo + pool_rows], preferred_element_type=jnp.float32)
        rounded = lax.optimization_barrier(partial_sum.astype(jnp.bfloat16))
        summed_out = summed_out + rounded.astype(jnp.float32)
    return summed_out.astype(jnp.bfloat16)

def reference(tokens, norm_gain, w_query, forget_weight, w_input, w_outgate, w_pool, forget_gap, extra_decay, rec_gain, group_weight, pool_gain, recurrent_output_weight, w_out_pool):
    weights = (norm_gain, w_query, forget_weight, w_input, w_outgate, w_pool, forget_gap, rec_gain, group_weight, pool_gain, recurrent_output_weight, w_out_pool)

    def per_sequence(pair):
        return one_sequence(pair[0], pair[1], weights)
    return lax.map(per_sequence, (tokens, extra_decay))
```

```python
import functools
import jax
import jax.numpy as jnp
from jax import lax
from jax.experimental import pallas as pl
from jax.experimental.pallas import tpu as pltpu
from jax.sharding import PartitionSpec as P

HEAD_DIM = 128
POOL_GROUPS = 4
BLOCK = 64
EPS = 1e-06
HIGH = lax.Precision.HIGHEST
MESH = pl.DeviceIdType.MESH
BF = jnp.bfloat16
F32 = jnp.float32


def place():
    return lax.axis_index("sp"), lax.axis_index("fs"), lax.axis_index("tp")


def rcopy(src, dst, ssem, rsem, dev):
    return pltpu.make_async_remote_copy(
        src_ref=src, dst_ref=dst, send_sem=ssem, recv_sem=rsem, device_id=dev, device_id_type=MESH
    )


def greet(devs):
    barrier = pltpu.get_barrier_semaphore()
    for cond, dev in devs:
        def tell(dev=dev):
            pl.semaphore_signal(barrier, inc=1, device_id=dev, device_id_type=MESH)
        if cond is None:
            tell()
        else:
            pl.when(cond)(tell)
    pl.semaphore_wait(barrier, sum(1 if cond is None else jnp.where(cond, 1, 0) for cond, _ in devs))


def project_kernel(
    n_sp, n_fs, n_tp, tok, wsrc, extra, gain, z_ref, e_ref,
    xs, ws, xs_send, xs_recv, d_send, d_recv, w_send, w_recv, zr_send, zl_send, e_send, e_recv,
):
    s, f, t = place()
    rows, half = tok.shape
    wr = wsrc.shape[1]
    other = (s, f, 1 - t)
    others = [lax.rem(f + d, n_fs) for d in range(1, n_fs)]
    up, down = (s + 1, f, t), (s - 1, f, t)
    has_up, has_down = s < n_sp - 1, s > 0
    greet([(None, other)] + [(None, (s, g, t)) for g in others] + [(has_up, up), (has_down, down)])

    def cols(c):
        return pl.ds(pl.multiple_of(c * half, half), half)

    def slot(a, b):
        return ws.at[pl.ds(pl.multiple_of((a * n_fs + b) * wr, wr), wr), :]

    def to_up(src, a, b):
        return rcopy(src, slot(a, b), zr_send.at[a, b], w_recv.at[a, b], up)

    def to_down(src, a, b):
        return rcopy(src, slot(a, b), zl_send.at[a, b], w_recv.at[a, b], down)

    own = wsrc.at[f]
    w_copies = [rcopy(wsrc.at[g], slot(s, f), w_send.at[d], w_recv.at[s, f], (s, g, t)) for d, g in enumerate(others)]
    for c in w_copies:
        c.start()
    pl.when(has_up)(lambda: to_up(own, s, f).start())
    pl.when(has_down)(lambda: to_down(own, s, f).start())
    x_copies = [rcopy(tok, xs.at[f, :, cols(t)], xs_send.at[d], xs_recv.at[f], (s, g, t)) for d, g in enumerate(others)]
    for c in x_copies:
        c.start()
    e_copies = [rcopy(extra.at[g], e_ref.at[f], e_send.at[d], e_recv.at[f], (s, g, t)) for d, g in enumerate(others)]
    for c in e_copies:
        c.start()
    first = rcopy(tok, xs.at[f, :, cols(t)], d_send.at[f], d_recv.at[f], other)
    first.start()
    ws[pl.ds(pl.multiple_of((s * n_fs + f) * wr, wr), wr), :] = wsrc[f]
    xs[f, :, cols(t)] = tok[...]
    e_ref[f] = extra[f]

    for g in others:
        to_up(slot(s, g), s, g).wait_recv()
        pl.when(has_up)(lambda: to_up(slot(s, g), s, g).start())
        pl.when(has_down)(lambda: to_down(slot(s, g), s, g).start())

    def swap(g):
        part = xs.at[g, :, cols(t)]
        return rcopy(part, part, d_send.at[g], d_recv.at[g], other)

    order = [f] + others

    def relay(d):
        for g in order:
            a = s - d

            @pl.when(a >= 0)
            def _():
                to_up(slot(a, g), a, g).wait_recv()
                pl.when(has_up)(lambda: to_up(slot(a, g), a, g).start())
            b = s + d

            @pl.when(b < n_sp)
            def _():
                to_down(slot(b, g), b, g).wait_recv()
                pl.when(has_down)(lambda: to_down(slot(b, g), b, g).start())

    def norm(g):
        theirs = xs.at[g, :, cols(1 - t)]
        rcopy(theirs, theirs, d_send.at[g], d_recv.at[g], other).wait_recv()
        step = 32
        for i in range(rows // step):
            feats = xs[g, pl.ds(i * step, step), :].astype(F32)
            scale = lax.rsqrt(jnp.mean(feats * feats, axis=-1, keepdims=True) + EPS)
            xs[g, pl.ds(i * step, step), :] = (feats * scale * gain[...]).astype(BF)

    relay(1)
    for i, g in enumerate(others):
        part = xs.at[g, :, cols(t)]
        rcopy(part, part, xs_send.at[i], xs_recv.at[g], other).wait_recv()
        swap(g).start()
    for d in range(2, n_sp):
        relay(d)
    for c in w_copies + x_copies + e_copies:
        c.wait_send()
    for g in others:
        rcopy(extra.at[f], e_ref.at[g], e_send.at[0], e_recv.at[g], other).wait_recv()
    first.wait_send()
    for g in others:
        swap(g).wait_send()
    for g in order:
        norm(g)

    def each(i, _):
        z_ref[i] = jnp.dot(xs[i], ws[...], preferred_element_type=F32).astype(BF)
        return 0

    lax.fori_loop(0, n_fs, each, 0)

    for d in range(n_sp):
        for g in order:
            a = s - d

            @pl.when((a >= 0) & has_up)
            def _():
                to_up(slot(a, g), a, g).wait_send()
            b = s + d

            @pl.when((b < n_sp) & has_down)
            def _():
                to_down(slot(b, g), b, g).wait_send()


def state_kernel(n_sp, state, decay, edge, st_out, de_out, ed_out, s_send, s_recv, c_send, c_recv, g_send, g_recv):
    s, f, t = place()
    devs = []
    for d in range(1, n_sp):
        devs.append((s + d < n_sp, (s + d, f, t)))
        devs.append((s - d >= 0, (s - d, f, t)))
    greet(devs)
    nxt = (s + 1, f, t)
    edge_copy = rcopy(edge, ed_out, g_send, g_recv, nxt)
    pl.when(s < n_sp - 1)(edge_copy.start)

    def pair(d):
        dev = (s + d, f, t)
        return (
            rcopy(state, st_out.at[d - 1], s_send.at[d - 1], s_recv.at[d - 1], dev),
            rcopy(decay, de_out.at[d - 1], c_send.at[d - 1], c_recv.at[d - 1], dev),
        )

    for d in range(1, n_sp):
        @pl.when(s + d < n_sp)
        def _():
            for c in pair(d):
                c.start()
    pl.when(s == 0)(lambda: ed_out.__setitem__(Ellipsis, jnp.zeros(ed_out.shape, ed_out.dtype)))
    for d in range(1, n_sp):
        @pl.when(s - d < 0)
        def _():
            st_out[d - 1] = jnp.zeros(st_out.shape[1:], st_out.dtype)
            de_out[d - 1] = jnp.ones(de_out.shape[1:], de_out.dtype)
    for d in range(1, n_sp):
        @pl.when(s - d >= 0)
        def _():
            for c in pair(d):
                c.wait_recv()
        @pl.when(s + d < n_sp)
        def _():
            for c in pair(d):
                c.wait_send()
    pl.when(s < n_sp - 1)(edge_copy.wait_send)
    pl.when(s > 0)(edge_copy.wait_recv)


def mix_kernel(
    n_sp, n_fs, n_tp, rec, pool, sq, ow, a_rec, a_pool, sq_out, ow_out,
    relay_buf, r_send, r_recv, p_send, p_recv, q_send, q_recv, dr_send, dr_recv, dp_send, dp_recv,
    up_send, down_send, o_recv, od_send, od_recv,
):
    s, f, t = place()
    n_half = n_sp // n_tp
    other = (s, f, 1 - t)
    others = [lax.rem(f + d, n_fs) for d in range(1, n_fs)]
    up, down = (s + 1, f, t), (s - 1, f, t)
    has_up, has_down = s < n_sp - 1, s > 0
    greet(
        [(None, other)] + [(None, (s, g, u)) for g in others for u in (t, 1 - t)] + [(has_up, up), (has_down, down)]
    )

    def cols(g, u):
        return pl.ds(pl.multiple_of((u * n_fs + g) * HEAD_DIM, HEAD_DIM), HEAD_DIM)

    def to_up(src, a):
        return rcopy(src, relay_buf.at[a], up_send.at[a], o_recv.at[a], up)

    def to_down(src, a):
        return rcopy(src, relay_buf.at[a], down_send.at[a], o_recv.at[a], down)

    def to_other(src, a):
        return rcopy(src, ow_out.at[lax.rem(a, n_half), t], od_send.at[a], od_recv.at[a], other)

    def keep(src, a):
        mine = a // n_half == t

        @pl.when(mine)
        def _():
            ow_out[lax.rem(a, n_half), t] = src[...]

        pl.when(jnp.logical_not(mine))(lambda: to_other(src, a).start())

    pl.when(has_up)(lambda: to_up(ow, s).start())
    pl.when(has_down)(lambda: to_down(ow, s).start())
    sends = []
    for d, g in enumerate(others):
        sends.append(rcopy(pool, a_pool.at[:, cols(f, t)], p_send.at[d], p_recv.at[f], (s, g, t)))
        sends.append(rcopy(rec, a_rec.at[:, cols(f, t)], r_send.at[d], r_recv.at[f], (s, g, t)))
        for u in range(n_tp):
            sends.append(rcopy(sq, sq_out.at[t, f], q_send.at[u, d], q_recv.at[t, f], (s, g, u)))
    sends.append(rcopy(pool, a_pool.at[:, cols(f, t)], dp_send.at[f], dp_recv.at[f], other))
    sends.append(rcopy(rec, a_rec.at[:, cols(f, t)], dr_send.at[f], dr_recv.at[f], other))
    sends.append(rcopy(sq, sq_out.at[t, f], q_send.at[0, n_fs - 1], q_recv.at[t, f], other))
    for c in sends:
        c.start()
    a_pool[:, cols(f, t)] = pool[...]
    a_rec[:, cols(f, t)] = rec[...]
    sq_out[t, f] = sq[...]
    keep(ow, s)
    for d, g in enumerate(others):
        for arr, rs, ds_, dr in ((a_pool, p_recv, dp_send, dp_recv), (a_rec, r_recv, dr_send, dr_recv)):
            part = arr.at[:, cols(g, t)]
            rcopy(part, part, ds_.at[g], rs.at[g], other).wait_recv()
            c = rcopy(part, part, ds_.at[g], dr.at[g], other)
            c.start()
            sends.append(c)
    for d in range(1, n_sp):
        a = s - d

        @pl.when(a >= 0)
        def _():
            to_up(relay_buf.at[a], a).wait_recv()
            pl.when(has_up)(lambda: to_up(relay_buf.at[a], a).start())
            keep(relay_buf.at[a], a)
        b = s + d

        @pl.when(b < n_sp)
        def _():
            to_down(relay_buf.at[b], b).wait_recv()
            pl.when(has_down)(lambda: to_down(relay_buf.at[b], b).start())
            keep(relay_buf.at[b], b)
    for g in [f] + others:
        for arr, ds_, dr in ((a_pool, dp_send, dp_recv), (a_rec, dr_send, dr_recv)):
            part = arr.at[:, cols(g, 1 - t)]
            rcopy(part, part, ds_.at[g], dr.at[g], other).wait_recv()
        for u in range(n_tp):
            here = sq_out.at[u, g]
            needed = rcopy(here, here, q_send.at[0, 0], q_recv.at[u, g], other)
            pl.when(jnp.logical_or(g != f, u != t))(needed.wait_recv)
    for i in range(n_half):
        a = t * n_half + i
        here = ow_out.at[i, 1 - t]
        rcopy(here, here, od_send.at[a], od_recv.at[a], other).wait_recv()
    for c in sends:
        c.wait_send()
    for i in range(n_half):
        a = (1 - t) * n_half + i
        to_other(ow, a).wait_send()
    for d in range(n_sp):
        a, b = s - d, s + d

        @pl.when((a >= 0) & has_up)
        def _():
            to_up(ow, a).wait_send()

        @pl.when((b < n_sp) & has_down)
        def _():
            to_down(ow, b).wait_send()


def spread_kernel(n_fs, n_tp, part, out, send, recv):
    s, f, t = place()
    others = [(lax.rem(f + d, n_fs), lax.rem(t + u, n_tp)) for d in range(n_fs) for u in range(n_tp)][1:]
    greet([(None, (s, g, u)) for g, u in others])
    copies = [
        rcopy(part.at[g, u], out.at[f, t], send.at[i], recv.at[f, t], (s, g, u)) for i, (g, u) in enumerate(others)
    ]
    for c in copies:
        c.start()
    out[f, t] = part[f, t]
    for c in copies:
        c.wait_send()
    for g, u in others:
        here = out.at[g, u]
        rcopy(here, here, send.at[0], recv.at[g, u], (s, g, u)).wait_recv()


def vmem(count):
    return [pl.BlockSpec(memory_space=pltpu.VMEM)] * count


def dma(*shape):
    return pltpu.SemaphoreType.DMA(shape) if shape else pltpu.SemaphoreType.DMA


def comm(kernel, outs, scratch, number, name):
    return pl.pallas_call(
        kernel,
        out_shape=[jax.ShapeDtypeStruct(a, b) for a, b in outs],
        out_specs=vmem(len(outs)),
        scratch_shapes=scratch,
        compiler_params=pltpu.CompilerParams(
            collective_id=number, has_side_effects=True, vmem_limit_bytes=60 * 1024 * 1024
        ),
        name=name,
    )


def local_recurrence(queries, input_gate, values, log_forget):
    tok_rows, head_count = (queries.shape[0], queries.shape[1])
    block_count = tok_rows // BLOCK
    q_blk, k_blk, v_blk, g_blk = (
        arr.reshape(block_count, BLOCK, head_count, HEAD_DIM)
        for arr in (queries, input_gate, values, log_forget)
    )
    within = jnp.cumsum(g_blk, axis=1)
    block_end = within[:, -1]
    q_up = q_blk * jnp.exp(within)
    k_down = k_blk * jnp.exp(-within)
    causal = jnp.tril(jnp.ones((BLOCK, BLOCK), jnp.bool_))
    scores = jnp.einsum("nthd,nshd->nhts", q_up, k_down, precision=HIGH)
    scores = jnp.where(causal, scores, 0.0)
    inner_out = jnp.einsum("nhts,nshe->nthe", scores, v_blk, precision=HIGH)
    updates = jnp.einsum(
        "nshd,nshe->nhde", k_blk * jnp.exp(block_end[:, None] - within), v_blk, precision=HIGH
    )
    decays = jnp.exp(block_end)
    state = jnp.zeros((head_count, HEAD_DIM, HEAD_DIM), F32)
    incoming = []
    for n in range(block_count):
        incoming.append(state)
        state = decays[n][:, :, None] * state + updates[n]
    offsets = jnp.cumsum(block_end, axis=0) - block_end
    total_log = jnp.sum(block_end, axis=0)
    return (inner_out, q_up, jnp.stack(incoming), jnp.exp(offsets), state, total_log)


def body(
    n_sp, n_fs, n_tp, tokens, norm_gain, w_query, forget_weight, w_input, w_outgate, w_pool, forget_gap,
    extra_decay, rec_gain, group_weight, pool_gain, recurrent_output_weight, w_out_pool,
):
    s, f, t = place()
    rows, half = tokens.shape[1:]
    width = w_query.shape[1]
    ch = width // n_fs
    n_w = 5
    wr = w_query.shape[0]
    stacked = jnp.stack(
        [w.reshape(wr, n_fs, ch) for w in (w_query, forget_weight, w_input, w_outgate, w_pool)], axis=2
    )
    wsrc = stacked.transpose(1, 0, 2, 3).reshape(n_fs, wr, n_w * ch)
    lanes = rows // 128
    extra = jnp.pad(extra_decay[0].T.reshape(n_fs, lanes, 128), ((0, 0), (0, 8 - lanes), (0, 0)))
    z, e_all = comm(
        functools.partial(project_kernel, n_sp, n_fs, n_tp),
        [((n_fs, rows, n_w * ch), BF), ((n_fs, 8, 128), F32)],
        [
            pltpu.VMEM((n_fs, rows, n_tp * half), BF), pltpu.VMEM((n_sp * n_fs * wr, n_w * ch), BF),
            dma(n_fs - 1), dma(n_fs), dma(n_fs), dma(n_fs), dma(n_fs - 1), dma(n_sp, n_fs),
            dma(n_sp, n_fs), dma(n_sp, n_fs), dma(n_fs - 1), dma(n_fs),
        ],
        1, "project",
    )(tokens[0], wsrc, extra, norm_gain[None])
    zf = z.astype(F32).transpose(1, 0, 2).reshape(rows, n_fs, n_w, ch)
    z_query, z_forget, z_input, z_outgate, z_pool = (zf[:, :, i] for i in range(n_w))
    gap = lax.dynamic_slice_in_dim(forget_gap, f * ch, ch, 0)
    gain = lax.dynamic_slice_in_dim(rec_gain, f * ch, ch, 0)
    decay_in = e_all[:, :lanes].reshape(n_fs, rows).T
    input_gate = gap * jax.nn.sigmoid(-z_forget)
    log_forget = jnp.log1p(-input_gate) + decay_in[:, :, None]
    inner_out, q_up, incoming, off, end_state, total_log = local_recurrence(
        jax.nn.silu(z_query), input_gate, z_input, log_forget
    )
    reach = 2**POOL_GROUPS
    tail = z[:, rows - reach :, (n_w - 1) * ch :]
    st, de, rim = comm(
        functools.partial(state_kernel, n_sp),
        [((n_sp - 1, n_fs, ch, ch), BF), ((n_sp - 1, n_fs, ch), F32), ((n_fs, reach, ch), BF)],
        [dma(n_sp - 1), dma(n_sp - 1), dma(n_sp - 1), dma(n_sp - 1), dma(), dma()],
        2, "state",
    )(end_state.astype(BF), jnp.exp(total_log), tail)
    total = jnp.zeros((n_fs, ch, ch), F32)
    for d in range(n_sp - 2, -1, -1):
        total = de[d][:, :, None] * total + st[d].astype(F32)
    entering = incoming + off[:, :, :, None] * total[None]
    recurrent = (inner_out + jnp.einsum("nthd,nhde->nthe", q_up, entering, precision=HIGH)).reshape(rows, n_fs, ch)
    square_sum = jnp.sum(recurrent * recurrent, axis=2)
    rec_act = (recurrent * gain * jax.nn.silu(z_outgate)).astype(BF).transpose(1, 0, 2).reshape(n_fs * rows, ch)
    sq = square_sum.T.reshape(n_fs * lanes, 128)

    zp = z[:, :, (n_w - 1) * ch :]
    running = jnp.concatenate([rim, zp], axis=1).astype(F32)
    group_dim = group_weight.shape[1]
    group = (t * width + f * ch) // group_dim
    window_total = None
    for level in range(POOL_GROUPS):
        stride = 2**level
        running = running[:, stride:] + running[:, :-stride]
        now = running[:, running.shape[1] - rows :]
        window_total = now if level == 0 else jnp.where(group == level, now, window_total)
    spot = s * rows + jnp.arange(rows, dtype=jnp.int32)
    counts = jnp.minimum(spot + 1, jnp.left_shift(jnp.int32(2), group)).astype(F32)
    pooled = (window_total / counts[None, :, None] - zp.astype(F32)).astype(BF).reshape(n_fs * rows, ch)

    groups_dev = w_out_pool.shape[0] // group_dim
    cw = w_out_pool.shape[1]
    local_map = lax.dynamic_slice_in_dim(group_weight, t * groups_dev, groups_dev, 0)
    scaled = (w_out_pool.astype(F32) * pool_gain[:, None]).astype(BF).reshape(groups_dev, group_dim, cw)
    folded = jnp.einsum("gcd,gdo->gco", local_map, scaled, preferred_element_type=F32).astype(BF)
    ow = jnp.concatenate(
        [recurrent_output_weight, folded.reshape(groups_dev * group_dim, cw)], axis=0
    ).reshape(-1, 128)
    n_half = n_sp // n_tp
    a_rec, a_pool, sq_all, ow_all = comm(
        functools.partial(mix_kernel, n_sp, n_fs, n_tp),
        [
            ((n_fs * rows, n_tp * width), BF), ((n_fs * rows, n_tp * width), BF),
            ((n_tp, n_fs) + sq.shape, F32), ((n_half, n_tp) + ow.shape, BF),
        ],
        [
            pltpu.VMEM((n_sp,) + ow.shape, BF),
            dma(n_fs - 1), dma(n_fs), dma(n_fs - 1), dma(n_fs), dma(n_tp, n_fs), dma(n_tp, n_fs),
            dma(n_fs), dma(n_fs), dma(n_fs), dma(n_fs),
            dma(n_sp), dma(n_sp), dma(n_sp), dma(n_sp), dma(n_sp),
        ],
        3, "mix",
    )(rec_act, pooled, sq, ow)
    ow_all = ow_all.reshape(n_half, n_tp, 2, width, cw)
    w_rec = ow_all[:, :, 0].transpose(1, 2, 0, 3).reshape(n_tp * width, n_half * cw)
    w_fold = ow_all[:, :, 1].transpose(1, 2, 0, 3).reshape(n_tp * width, n_half * cw)
    total_sq = jnp.sum(sq_all, axis=(0, 1)).reshape(n_fs * rows, 1)
    rec_scale = lax.rsqrt(total_sq / (n_tp * width) + EPS)
    mixed = (
        jnp.dot(a_rec, w_rec, preferred_element_type=F32) * rec_scale
        + jnp.dot(a_pool, w_fold, preferred_element_type=F32)
    ).astype(BF)
    mixed = mixed.reshape(n_fs, n_tp, rows // n_tp, n_half * cw)
    (final,) = comm(
        functools.partial(spread_kernel, n_fs, n_tp),
        [(mixed.shape, BF)],
        [dma(n_fs * n_tp), dma(n_fs, n_tp)],
        4, "spread",
    )(mixed)
    final = final.reshape(n_fs, n_tp, rows // n_tp, n_half, cw).transpose(2, 1, 3, 0, 4)
    return final.reshape(1, rows // n_tp, n_tp * n_half * n_fs * cw)


def solution(mesh):
    sizes = dict(mesh.shape)
    weight = P(("sp", "fs"), "tp")
    placed = (
        P("fs", "sp", "tp"), P(), weight, weight, weight, weight, weight, P("tp"),
        P("fs", "sp", "tp"), P("tp"), P(), P("tp"), P("tp", ("sp", "fs")), P("tp", ("sp", "fs")),
    )
    return jax.shard_map(
        functools.partial(body, sizes["sp"], sizes["fs"], sizes["tp"]),
        mesh=mesh, in_specs=placed, out_specs=P("fs", ("sp", "tp"), None), check_vma=False,
    )
```

```python
import functools
import jax
import jax.numpy as jnp
from jax import lax
from jax.experimental import pallas as pl
from jax.experimental.pallas import tpu as pltpu
from jax.sharding import PartitionSpec as P

HEAD_DIM = 128
POOL_GROUPS = 4
BLOCK = 64
EPS = 1e-06
HIGH = lax.Precision.HIGHEST
MESH = pl.DeviceIdType.MESH
BF = jnp.bfloat16
F32 = jnp.float32


def place():
    return lax.axis_index("sp"), lax.axis_index("fs"), lax.axis_index("tp")


def rcopy(src, dst, ssem, rsem, dev):
    return pltpu.make_async_remote_copy(
        src_ref=src, dst_ref=dst, send_sem=ssem, recv_sem=rsem, device_id=dev, device_id_type=MESH
    )


def greet(devs):
    barrier = pltpu.get_barrier_semaphore()
    for cond, dev in devs:
        def tell(dev=dev):
            pl.semaphore_signal(barrier, inc=1, device_id=dev, device_id_type=MESH)
        if cond is None:
            tell()
        else:
            pl.when(cond)(tell)
    pl.semaphore_wait(barrier, sum(1 if cond is None else jnp.where(cond, 1, 0) for cond, _ in devs))


def project_kernel(
    n_sp, n_fs, n_tp, tok, wsrc, extra, gain, z_ref, e_ref,
    xs, ws, xs_send, xs_recv, d_send, d_recv, w_send, w_recv, zr_send, zl_send, e_send, e_recv,
):
    s, f, t = place()
    rows, half = tok.shape
    wr = wsrc.shape[1]
    other = (s, f, 1 - t)
    others = [lax.rem(f + d, n_fs) for d in range(1, n_fs)]
    up, down = (s + 1, f, t), (s - 1, f, t)
    has_up, has_down = s < n_sp - 1, s > 0
    greet([(None, other)] + [(None, (s, g, t)) for g in others] + [(has_up, up), (has_down, down)])

    def cols(c):
        return pl.ds(pl.multiple_of(c * half, half), half)

    def slot(a, b):
        return ws.at[pl.ds(pl.multiple_of((a * n_fs + b) * wr, wr), wr), :]

    def to_up(src, a, b):
        return rcopy(src, slot(a, b), zr_send.at[a, b], w_recv.at[a, b], up)

    def to_down(src, a, b):
        return rcopy(src, slot(a, b), zl_send.at[a, b], w_recv.at[a, b], down)

    own = wsrc.at[f]
    w_copies = [rcopy(wsrc.at[g], slot(s, f), w_send.at[d], w_recv.at[s, f], (s, g, t)) for d, g in enumerate(others)]
    for c in w_copies:
        c.start()
    pl.when(has_up)(lambda: to_up(own, s, f).start())
    pl.when(has_down)(lambda: to_down(own, s, f).start())
    x_copies = [rcopy(tok, xs.at[f, :, cols(t)], xs_send.at[d], xs_recv.at[f], (s, g, t)) for d, g in enumerate(others)]
    for c in x_copies:
        c.start()
    e_copies = [rcopy(extra.at[g], e_ref.at[f], e_send.at[d], e_recv.at[f], (s, g, t)) for d, g in enumerate(others)]
    for c in e_copies:
        c.start()
    first = rcopy(tok, xs.at[f, :, cols(t)], d_send.at[f], d_recv.at[f], other)
    first.start()
    ws[pl.ds(pl.multiple_of((s * n_fs + f) * wr, wr), wr), :] = wsrc[f]
    xs[f, :, cols(t)] = tok[...]
    e_ref[f] = extra[f]

    for g in others:
        to_up(slot(s, g), s, g).wait_recv()
        pl.when(has_up)(lambda: to_up(slot(s, g), s, g).start())
        pl.when(has_down)(lambda: to_down(slot(s, g), s, g).start())

    def swap(g):
        part = xs.at[g, :, cols(t)]
        return rcopy(part, part, d_send.at[g], d_recv.at[g], other)

    order = [f] + others

    def relay(d):
        for g in order:
            a = s - d

            @pl.when(a >= 0)
            def _():
                to_up(slot(a, g), a, g).wait_recv()
                pl.when(has_up)(lambda: to_up(slot(a, g), a, g).start())
            b = s + d

            @pl.when(b < n_sp)
            def _():
                to_down(slot(b, g), b, g).wait_recv()
                pl.when(has_down)(lambda: to_down(slot(b, g), b, g).start())

    def norm(g):
        theirs = xs.at[g, :, cols(1 - t)]
        rcopy(theirs, theirs, d_send.at[g], d_recv.at[g], other).wait_recv()
        step = 32
        for i in range(rows // step):
            feats = xs[g, pl.ds(i * step, step), :].astype(F32)
            scale = lax.rsqrt(jnp.mean(feats * feats, axis=-1, keepdims=True) + EPS)
            xs[g, pl.ds(i * step, step), :] = (feats * scale * gain[...]).astype(BF)

    relay(1)
    for i, g in enumerate(others):
        part = xs.at[g, :, cols(t)]
        rcopy(part, part, xs_send.at[i], xs_recv.at[g], other).wait_recv()
        swap(g).start()
    for d in range(2, n_sp):
        relay(d)
    for c in w_copies + x_copies + e_copies:
        c.wait_send()
    for g in others:
        rcopy(extra.at[f], e_ref.at[g], e_send.at[0], e_recv.at[g], other).wait_recv()
    first.wait_send()
    for g in others:
        swap(g).wait_send()
    for g in order:
        norm(g)

    def each(i, _):
        z_ref[i] = jnp.dot(xs[i], ws[...], preferred_element_type=F32).astype(BF)
        return 0

    lax.fori_loop(0, n_fs, each, 0)

    for d in range(n_sp):
        for g in order:
            a = s - d

            @pl.when((a >= 0) & has_up)
            def _():
                to_up(slot(a, g), a, g).wait_send()
            b = s + d

            @pl.when((b < n_sp) & has_down)
            def _():
                to_down(slot(b, g), b, g).wait_send()


def state_kernel(n_sp, state, decay, edge, st_out, de_out, ed_out, s_send, s_recv, c_send, c_recv, g_send, g_recv):
    s, f, t = place()
    devs = []
    for d in range(1, n_sp):
        devs.append((s + d < n_sp, (s + d, f, t)))
        devs.append((s - d >= 0, (s - d, f, t)))
    greet(devs)
    nxt = (s + 1, f, t)
    edge_copy = rcopy(edge, ed_out, g_send, g_recv, nxt)
    pl.when(s < n_sp - 1)(edge_copy.start)

    def pair(d):
        dev = (s + d, f, t)
        return (
            rcopy(state, st_out.at[d - 1], s_send.at[d - 1], s_recv.at[d - 1], dev),
            rcopy(decay, de_out.at[d - 1], c_send.at[d - 1], c_recv.at[d - 1], dev),
        )

    for d in range(1, n_sp):
        @pl.when(s + d < n_sp)
        def _():
            for c in pair(d):
                c.start()
    pl.when(s == 0)(lambda: ed_out.__setitem__(Ellipsis, jnp.zeros(ed_out.shape, ed_out.dtype)))
    for d in range(1, n_sp):
        @pl.when(s - d < 0)
        def _():
            st_out[d - 1] = jnp.zeros(st_out.shape[1:], st_out.dtype)
            de_out[d - 1] = jnp.ones(de_out.shape[1:], de_out.dtype)
    for d in range(1, n_sp):
        @pl.when(s - d >= 0)
        def _():
            for c in pair(d):
                c.wait_recv()
        @pl.when(s + d < n_sp)
        def _():
            for c in pair(d):
                c.wait_send()
    pl.when(s < n_sp - 1)(edge_copy.wait_send)
    pl.when(s > 0)(edge_copy.wait_recv)


def square(f):
    near = f + 1 - 2 * lax.rem(f, 2)
    return near, lax.rem(f + 2, 4), lax.rem(near + 2, 4)


def mix_kernel(
    n_sp, n_fs, n_tp, act, sq, ow, out,
    acts, sq_all, ow_all, relay_buf, wbuf, part,
    a_send, a_recv, f_send, d_send, d_recv, q_send, q_recv,
    up_send, down_send, o_recv, od_send, od_recv, m_send, m_recv,
):
    s, f, t = place()
    n_half = n_sp // n_tp
    rows = act.shape[1] // n_fs
    half = rows // n_tp
    width, cw = ow.shape[0] // 2, ow.shape[1]
    other = (s, f, 1 - t)
    px, py, pd = square(f)
    up, down = (s + 1, f, t), (s - 1, f, t)
    has_up, has_down = s < n_sp - 1, s > 0
    greet(
        [(None, other)]
        + [(None, (s, g, u)) for g in (px, py, pd) for u in (t, 1 - t)]
        + [(has_up, up), (has_down, down)]
    )

    def to_up(src, a):
        return rcopy(src, relay_buf.at[a], up_send.at[a], o_recv.at[a], up)

    def to_down(src, a):
        return rcopy(src, relay_buf.at[a], down_send.at[a], o_recv.at[a], down)

    def to_other(src, a):
        return rcopy(src, ow_all.at[lax.rem(a, n_half), t], od_send.at[a], od_recv.at[a], other)

    def keep(src, a):
        mine = a // n_half == t

        @pl.when(mine)
        def _():
            ow_all[lax.rem(a, n_half), t] = src[...]

        pl.when(jnp.logical_not(mine))(lambda: to_other(src, a).start())

    sends = []

    def send(c):
        c.start()
        sends.append(c)

    for i, (p, order) in enumerate(((px, (0, 1)), (py, (1, 0)))):
        for h in order:
            send(rcopy(act.at[h], acts.at[t, f, h], a_send.at[i, h], a_recv.at[f, h], (s, p, t)))
    pl.when(has_up)(lambda: to_up(ow, s).start())
    pl.when(has_down)(lambda: to_down(ow, s).start())
    for h in range(2):
        send(rcopy(act.at[h], acts.at[t, f, h], d_send.at[f, h], d_recv.at[f, h], other))
    for i, g in enumerate((px, py, pd)):
        for u in range(n_tp):
            send(rcopy(sq, sq_all.at[t, f], q_send.at[i, u], q_recv.at[t, f], (s, g, u)))
    send(rcopy(sq, sq_all.at[t, f], q_send.at[n_fs - 1, 0], q_recv.at[t, f], other))
    acts[t, f] = act[...]
    sq_all[t, f] = sq[...]
    keep(ow, s)

    def landed(g, h):
        here = acts.at[t, g, h]
        rcopy(here, here, d_send.at[g, h], a_recv.at[g, h], other).wait_recv()
        return here

    def hand_on(g, h, here):
        send(rcopy(here, here, d_send.at[g, h], d_recv.at[g, h], other))

    for i, (g, h, onto) in enumerate(((px, 0, py), (py, 1, px))):
        here = landed(g, h)
        send(rcopy(here, here, f_send.at[i], a_recv.at[g, h], (s, onto, t)))
        hand_on(g, h, here)

    def step(d):
        a = s - d

        @pl.when(a >= 0)
        def _():
            to_up(relay_buf.at[a], a).wait_recv()
            pl.when(has_up)(lambda: to_up(relay_buf.at[a], a).start())
            keep(relay_buf.at[a], a)
        b = s + d

        @pl.when(b < n_sp)
        def _():
            to_down(relay_buf.at[b], b).wait_recv()
            pl.when(has_down)(lambda: to_down(relay_buf.at[b], b).start())
            keep(relay_buf.at[b], b)

    for d in range(1, n_sp):
        step(d)
    for g, h in ((px, 1), (py, 0), (pd, 0), (pd, 1)):
        hand_on(g, h, landed(g, h))
    for i in range(n_half):
        a = t * n_half + i
        here = ow_all.at[i, 1 - t]
        rcopy(here, here, od_send.at[a], od_recv.at[a], other).wait_recv()
    for i in range(n_half):
        for u in range(n_tp):
            for k in range(2):
                wbuf[k, u * width : (u + 1) * width, i * cw : (i + 1) * cw] = ow_all[i, u, k * width : (k + 1) * width, :]
    for g in (px, py, pd):
        for u in range(n_tp):
            here = sq_all.at[u, g]
            rcopy(here, here, q_send.at[0, 0], q_recv.at[u, g], other).wait_recv()
    here = sq_all.at[1 - t, f]
    rcopy(here, here, q_send.at[0, 0], q_recv.at[1 - t, f], other).wait_recv()
    for g in (f, px, py, pd):
        for h in range(2):
            here = acts.at[1 - t, g, h]
            rcopy(here, here, d_send.at[g, h], d_recv.at[g, h], other).wait_recv()

    def piece(g, u):
        return rcopy(part.at[g, u], out.at[f, t], m_send.at[g, u], m_recv.at[f, t], (s, g, u))

    def spread(g):
        for u in range(n_tp):
            c = piece(g, u)
            c.start()
            sends.append(c)

    last = None
    for g in (pd, f, px, py):
        here = pl.ds(pl.multiple_of(g * rows, rows), rows)
        sums = sum(sq_all[u, i, g] for u in range(n_tp) for i in range(n_fs))
        scale = lax.rsqrt(sums / (n_tp * width) + EPS).T
        scale = jnp.concatenate([scale[:, i : i + 1] for i in range(rows // 128)], axis=0)
        left = [
            jnp.concatenate([acts[u, i, h, here, :] for u in range(n_tp) for i in range(n_fs)], axis=1)
            for h in range(2)
        ]
        mixed = (
            jnp.dot(left[0], wbuf[0], preferred_element_type=F32) * scale
            + jnp.dot(left[1], wbuf[1], preferred_element_type=F32)
        ).astype(BF)
        for u in range(n_tp):
            part[g, u] = mixed[u * half : (u + 1) * half]
        if last is not None and last is not f:
            spread(last)
        if last is f:
            c = piece(f, 1 - t)
            c.start()
            sends.append(c)
        last = g
    out[f, t] = part[f, t]
    for i in range(n_half):
        to_other(ow, (1 - t) * n_half + i).wait_send()
    for d in range(n_sp):
        a, b = s - d, s + d

        @pl.when((a >= 0) & has_up)
        def _():
            to_up(ow, a).wait_send()

        @pl.when((b < n_sp) & has_down)
        def _():
            to_down(ow, b).wait_send()
    spread(last)
    for c in sends:
        c.wait_send()
    for g in (px, py, pd):
        for u in range(n_tp):
            here = out.at[g, u]
            rcopy(here, here, m_send.at[g, u], m_recv.at[g, u], other).wait_recv()
    here = out.at[f, 1 - t]
    rcopy(here, here, m_send.at[f, 1 - t], m_recv.at[f, 1 - t], other).wait_recv()


def vmem(count):
    return [pl.BlockSpec(memory_space=pltpu.VMEM)] * count


def dma(*shape):
    return pltpu.SemaphoreType.DMA(shape) if shape else pltpu.SemaphoreType.DMA


def comm(kernel, outs, scratch, number, name):
    return pl.pallas_call(
        kernel,
        out_shape=[jax.ShapeDtypeStruct(a, b) for a, b in outs],
        out_specs=vmem(len(outs)),
        scratch_shapes=scratch,
        compiler_params=pltpu.CompilerParams(
            collective_id=number, has_side_effects=True, vmem_limit_bytes=60 * 1024 * 1024
        ),
        name=name,
    )


def local_recurrence(queries, input_gate, values, log_forget):
    tok_rows, head_count = (queries.shape[0], queries.shape[1])
    block_count = tok_rows // BLOCK
    q_blk, k_blk, v_blk, g_blk = (
        arr.reshape(block_count, BLOCK, head_count, HEAD_DIM)
        for arr in (queries, input_gate, values, log_forget)
    )
    within = jnp.cumsum(g_blk, axis=1)
    block_end = within[:, -1]
    q_up = q_blk * jnp.exp(within)
    k_down = k_blk * jnp.exp(-within)
    causal = jnp.tril(jnp.ones((BLOCK, BLOCK), jnp.bool_))
    scores = jnp.einsum("nthd,nshd->nhts", q_up, k_down, precision=HIGH)
    scores = jnp.where(causal, scores, 0.0)
    inner_out = jnp.einsum("nhts,nshe->nthe", scores, v_blk, precision=HIGH)
    updates = jnp.einsum(
        "nshd,nshe->nhde", k_blk * jnp.exp(block_end[:, None] - within), v_blk, precision=HIGH
    )
    decays = jnp.exp(block_end)
    state = jnp.zeros((head_count, HEAD_DIM, HEAD_DIM), F32)
    incoming = []
    for n in range(block_count):
        incoming.append(state)
        state = decays[n][:, :, None] * state + updates[n]
    offsets = jnp.cumsum(block_end, axis=0) - block_end
    total_log = jnp.sum(block_end, axis=0)
    return (inner_out, q_up, jnp.stack(incoming), jnp.exp(offsets), state, total_log)


def body(
    n_sp, n_fs, n_tp, tokens, norm_gain, w_query, forget_weight, w_input, w_outgate, w_pool, forget_gap,
    extra_decay, rec_gain, group_weight, pool_gain, recurrent_output_weight, w_out_pool,
):
    s, f, t = place()
    rows, half = tokens.shape[1:]
    width = w_query.shape[1]
    ch = width // n_fs
    n_w = 5
    wr = w_query.shape[0]
    stacked = jnp.stack(
        [w.reshape(wr, n_fs, ch) for w in (w_query, forget_weight, w_input, w_outgate, w_pool)], axis=2
    )
    wsrc = stacked.transpose(1, 0, 2, 3).reshape(n_fs, wr, n_w * ch)
    lanes = rows // 128
    extra = jnp.pad(extra_decay[0].T.reshape(n_fs, lanes, 128), ((0, 0), (0, 8 - lanes), (0, 0)))
    z, e_all = comm(
        functools.partial(project_kernel, n_sp, n_fs, n_tp),
        [((n_fs, rows, n_w * ch), BF), ((n_fs, 8, 128), F32)],
        [
            pltpu.VMEM((n_fs, rows, n_tp * half), BF), pltpu.VMEM((n_sp * n_fs * wr, n_w * ch), BF),
            dma(n_fs - 1), dma(n_fs), dma(n_fs), dma(n_fs), dma(n_fs - 1), dma(n_sp, n_fs),
            dma(n_sp, n_fs), dma(n_sp, n_fs), dma(n_fs - 1), dma(n_fs),
        ],
        1, "project",
    )(tokens[0], wsrc, extra, norm_gain[None])
    zf = z.astype(F32).transpose(1, 0, 2).reshape(rows, n_fs, n_w, ch)
    z_query, z_forget, z_input, z_outgate, z_pool = (zf[:, :, i] for i in range(n_w))
    gap = lax.dynamic_slice_in_dim(forget_gap, f * ch, ch, 0)
    gain = lax.dynamic_slice_in_dim(rec_gain, f * ch, ch, 0)
    decay_in = e_all[:, :lanes].reshape(n_fs, rows).T
    input_gate = gap * jax.nn.sigmoid(-z_forget)
    log_forget = jnp.log1p(-input_gate) + decay_in[:, :, None]
    inner_out, q_up, incoming, off, end_state, total_log = local_recurrence(
        jax.nn.silu(z_query), input_gate, z_input, log_forget
    )
    reach = 2**POOL_GROUPS
    tail = z[:, rows - reach :, (n_w - 1) * ch :]
    st, de, rim = comm(
        functools.partial(state_kernel, n_sp),
        [((n_sp - 1, n_fs, ch, ch), BF), ((n_sp - 1, n_fs, ch), F32), ((n_fs, reach, ch), BF)],
        [dma(n_sp - 1), dma(n_sp - 1), dma(n_sp - 1), dma(n_sp - 1), dma(), dma()],
        2, "state",
    )(end_state.astype(BF), jnp.exp(total_log), tail)
    total = jnp.zeros((n_fs, ch, ch), F32)
    for d in range(n_sp - 2, -1, -1):
        total = de[d][:, :, None] * total + st[d].astype(F32)
    entering = incoming + off[:, :, :, None] * total[None]
    recurrent = (inner_out + jnp.einsum("nthd,nhde->nthe", q_up, entering, precision=HIGH)).reshape(rows, n_fs, ch)
    square_sum = jnp.sum(recurrent * recurrent, axis=2)
    rec_act = (recurrent * gain * jax.nn.silu(z_outgate)).astype(BF).transpose(1, 0, 2).reshape(n_fs * rows, ch)
    sq = jnp.pad(square_sum.T.reshape(n_fs, lanes, 128), ((0, 0), (0, 8 - lanes), (0, 0)))

    zp = z[:, :, (n_w - 1) * ch :]
    running = jnp.concatenate([rim, zp], axis=1).astype(F32)
    group_dim = group_weight.shape[1]
    group = (t * width + f * ch) // group_dim
    window_total = None
    for level in range(POOL_GROUPS):
        stride = 2**level
        running = running[:, stride:] + running[:, :-stride]
        now = running[:, running.shape[1] - rows :]
        window_total = now if level == 0 else jnp.where(group == level, now, window_total)
    spot = s * rows + jnp.arange(rows, dtype=jnp.int32)
    counts = jnp.minimum(spot + 1, jnp.left_shift(jnp.int32(2), group)).astype(F32)
    pooled = (window_total / counts[None, :, None] - zp.astype(F32)).astype(BF).reshape(n_fs * rows, ch)

    groups_dev = w_out_pool.shape[0] // group_dim
    cw = w_out_pool.shape[1]
    local_map = lax.dynamic_slice_in_dim(group_weight, t * groups_dev, groups_dev, 0)
    scaled = (w_out_pool.astype(F32) * pool_gain[:, None]).astype(BF).reshape(groups_dev, group_dim, cw)
    folded = jnp.einsum("gcd,gdo->gco", local_map, scaled, preferred_element_type=F32).astype(BF)
    ow = jnp.concatenate([recurrent_output_weight, folded.reshape(groups_dev * group_dim, cw)], axis=0)
    n_half = n_sp // n_tp
    act = jnp.stack([rec_act, pooled])
    out_shape = (n_fs, n_tp, rows // n_tp, n_half * cw)
    (final,) = comm(
        functools.partial(mix_kernel, n_sp, n_fs, n_tp),
        [(out_shape, BF)],
        [
            pltpu.VMEM((n_tp, n_fs) + act.shape, BF), pltpu.VMEM((n_tp, n_fs) + sq.shape, F32),
            pltpu.VMEM((n_half, n_tp) + ow.shape, BF), pltpu.VMEM((n_sp,) + ow.shape, BF),
            pltpu.VMEM((2, n_tp * width, n_half * cw), BF), pltpu.VMEM(out_shape, BF),
            dma(2, 2), dma(n_fs, 2), dma(2), dma(n_fs, 2), dma(n_fs, 2), dma(n_fs, n_tp), dma(n_tp, n_fs),
            dma(n_sp), dma(n_sp), dma(n_sp), dma(n_sp), dma(n_sp), dma(n_fs, n_tp), dma(n_fs, n_tp),
        ],
        3, "mix",
    )(act, sq, ow)
    final = final.reshape(n_fs, n_tp, rows // n_tp, n_half, cw).transpose(2, 1, 3, 0, 4)
    return final.reshape(1, rows // n_tp, n_tp * n_half * n_fs * cw)


def solution(mesh):
    sizes = dict(mesh.shape)
    weight = P(("sp", "fs"), "tp")
    placed = (
        P("fs", "sp", "tp"), P(), weight, weight, weight, weight, weight, P("tp"),
        P("fs", "sp", "tp"), P("tp"), P(), P("tp"), P("tp", ("sp", "fs")), P("tp", ("sp", "fs")),
    )
    return jax.shard_map(
        functools.partial(body, sizes["sp"], sizes["fs"], sizes["tp"]),
        mesh=mesh, in_specs=placed, out_specs=P("fs", ("sp", "tp"), None), check_vma=False,
    )
```

```python
import functools
import jax
import jax.numpy as jnp
from jax import lax
from jax.experimental import pallas as pl
from jax.experimental.pallas import tpu as pltpu
from jax.sharding import PartitionSpec as P

HEAD_DIM = 128
POOL_GROUPS = 4
BLOCK = 64
EPS = 1e-06
HIGH = lax.Precision.HIGHEST
MESH = pl.DeviceIdType.MESH
BF = jnp.bfloat16
F32 = jnp.float32


def place():
    return lax.axis_index("sp"), lax.axis_index("fs"), lax.axis_index("tp")


def rcopy(src, dst, ssem, rsem, dev):
    return pltpu.make_async_remote_copy(
        src_ref=src, dst_ref=dst, send_sem=ssem, recv_sem=rsem, device_id=dev, device_id_type=MESH
    )


def greet(devs):
    barrier = pltpu.get_barrier_semaphore()
    for cond, dev in devs:
        def tell(dev=dev):
            pl.semaphore_signal(barrier, inc=1, device_id=dev, device_id_type=MESH)
        if cond is None:
            tell()
        else:
            pl.when(cond)(tell)
    pl.semaphore_wait(barrier, sum(1 if cond is None else jnp.where(cond, 1, 0) for cond, _ in devs))


def square(f):
    near = f + 1 - 2 * lax.rem(f, 2)
    return near, lax.rem(f + 2, 4), lax.rem(near + 2, 4)


def project_kernel(
    n_sp, n_fs, n_tp, tok, wq, wf, wi, wo, wp, extra, gain, gmap, pgain, wor, wop, z_ref, e_ref, ow_ref,
    wsrc, xs, ws, acc, x_send, x_recv, f_send, d_send, d_recv, w_send, w_recv, zr_send, zl_send, e_send, e_recv,
):
    s, f, t = place()
    rows, half = tok.shape
    part = rows // 2
    mats = (wq, wf, wi, wo, wp)
    wr, width = wq.shape
    ch = width // n_fs
    for i, w in enumerate(mats):
        for g in range(n_fs):
            wsrc[g, :, i * ch : (i + 1) * ch] = w[:, g * ch : (g + 1) * ch]
    other = (s, f, 1 - t)
    px, py, pd = square(f)
    order = (f, px, py, pd)
    up, down = (s + 1, f, t), (s - 1, f, t)
    has_up, has_down = s < n_sp - 1, s > 0
    greet([(None, other)] + [(None, (s, g, t)) for g in order[1:]] + [(has_up, up), (has_down, down)])

    def cols(c):
        return pl.ds(pl.multiple_of(c * half, half), half)

    def span(a, b):
        return pl.ds(pl.multiple_of((a * n_fs + b) * wr, wr), wr)

    def slot(a, b):
        return ws.at[span(a, b), :]

    def to_up(src, a, b):
        return rcopy(src, slot(a, b), zr_send.at[a, b], w_recv.at[a, b], up)

    def to_down(src, a, b):
        return rcopy(src, slot(a, b), zl_send.at[a, b], w_recv.at[a, b], down)

    sends = []

    def send(c):
        c.start()
        sends.append(c)

    def x_slot(g, h, c):
        return xs.at[g, h * part : (h + 1) * part, cols(c)]

    own = wsrc.at[f]
    pl.when(has_up)(lambda: to_up(own, s, f).start())
    pl.when(has_down)(lambda: to_down(own, s, f).start())
    for i, g in enumerate((pd, px, py)):
        send(rcopy(wsrc.at[g], slot(s, f), w_send.at[i], w_recv.at[s, f], (s, g, t)))
    for i, (p, hs) in enumerate(((px, (0, 1)), (py, (1, 0)))):
        for h in hs:
            send(rcopy(tok.at[h * part : (h + 1) * part, :], x_slot(f, h, t), x_send.at[i, h], x_recv.at[f, h], (s, p, t)))
    for h in range(2):
        send(rcopy(tok.at[h * part : (h + 1) * part, :], x_slot(f, h, t), d_send.at[f, h], d_recv.at[f, h], other))
    for i, g in enumerate(order[1:]):
        send(rcopy(extra.at[g], e_ref.at[f], e_send.at[i], e_recv.at[f], (s, g, t)))
    ws[span(s, f), :] = wsrc[f]
    xs[f, :, cols(t)] = tok[...]
    e_ref[f] = extra[f]
    ow_ref[0:width, :] = wor[...]
    gd = gmap.shape[1]
    for i in range(width // gd):
        at = slice(i * gd, (i + 1) * gd)
        scaled = (gmap[t * (width // gd) + i].astype(F32) * pgain[:, at]).astype(BF)
        folded = jnp.dot(scaled, wop[at, :], preferred_element_type=F32)
        ow_ref[width + i * gd : width + (i + 1) * gd, :] = folded.astype(BF)

    for g in order[1:]:
        to_up(slot(s, g), s, g).wait_recv()
        pl.when(has_up)(lambda: to_up(slot(s, g), s, g).start())
        pl.when(has_down)(lambda: to_down(slot(s, g), s, g).start())

    def landed(g, h):
        here = x_slot(g, h, t)
        rcopy(here, here, d_send.at[g, h], x_recv.at[g, h], other).wait_recv()
        return here

    def hand_on(g, h, here):
        send(rcopy(here, here, d_send.at[g, h], d_recv.at[g, h], other))

    for i, (g, h, onto) in enumerate(((px, 0, py), (py, 1, px))):
        here = landed(g, h)
        send(rcopy(here, here, f_send.at[i], x_recv.at[g, h], (s, onto, t)))
        hand_on(g, h, here)

    def relay(d):
        for g in order:
            a = s - d

            @pl.when(a >= 0)
            def _():
                to_up(slot(a, g), a, g).wait_recv()
                pl.when(has_up)(lambda: to_up(slot(a, g), a, g).start())
            b = s + d

            @pl.when(b < n_sp)
            def _():
                to_down(slot(b, g), b, g).wait_recv()
                pl.when(has_down)(lambda: to_down(slot(b, g), b, g).start())

    def add(a):
        k = pl.ds(pl.multiple_of(a * n_fs * wr, n_fs * wr), n_fs * wr)

        def each(i, _):
            acc[i] += jnp.dot(xs[i, :, k], ws[k, :], preferred_element_type=F32)
            return 0

        lax.fori_loop(0, n_fs, each, 0)

    def multiply(d):
        pl.when(s - d >= 0)(lambda: add(s - d))
        pl.when(s + d < n_sp)(lambda: add(s + d))

    relay(1)
    for g, h in ((px, 1), (py, 0), (pd, 0), (pd, 1)):
        hand_on(g, h, landed(g, h))
    for d in range(2, n_sp - 1):
        relay(d)
    for g in order:
        for h in range(2):
            here = x_slot(g, h, 1 - t)
            rcopy(here, here, d_send.at[g, h], d_recv.at[g, h], other).wait_recv()
    for g in order[1:]:
        rcopy(extra.at[f], e_ref.at[g], e_send.at[0], e_recv.at[g], other).wait_recv()
    for c in sends:
        c.wait_send()

    def norm(j, _):
        tile = 16
        per = rows // tile
        at = (j // per, pl.ds(pl.multiple_of(lax.rem(j, per) * tile, tile), tile))
        feats = xs[at[0], at[1], :].astype(F32)
        scale = lax.rsqrt(jnp.mean(feats * feats, axis=-1, keepdims=True) + EPS)
        xs[at[0], at[1], :] = (feats * scale * gain[...]).astype(BF)
        return 0

    lax.fori_loop(0, n_fs * rows // 16, norm, 0, unroll=2)

    if n_fs * wr % 128 == 0:
        own_k = pl.ds(pl.multiple_of(s * n_fs * wr, n_fs * wr), n_fs * wr)

        def begin(i, _):
            acc[i] = jnp.dot(xs[i, :, own_k], ws[own_k, :], preferred_element_type=F32)
            return 0

        lax.fori_loop(0, n_fs, begin, 0)
        for d in range(1, n_sp - 1):
            multiply(d)
        relay(n_sp - 1)
        multiply(n_sp - 1)

        def finish(i, _):
            z_ref[i] = acc[i].astype(BF)
            return 0
    else:
        relay(n_sp - 1)

        def finish(i, _):
            z_ref[i] = jnp.dot(xs[i], ws[...], preferred_element_type=F32).astype(BF)
            return 0

    lax.fori_loop(0, n_fs, finish, 0)

    for d in range(n_sp):
        for g in order:
            a = s - d

            @pl.when((a >= 0) & has_up)
            def _():
                to_up(slot(a, g), a, g).wait_send()
            b = s + d

            @pl.when((b < n_sp) & has_down)
            def _():
                to_down(slot(b, g), b, g).wait_send()


def state_kernel(n_sp, state, decay, edge, st_out, de_out, ed_out, s_send, s_recv, c_send, c_recv, g_send, g_recv):
    s, f, t = place()
    devs = []
    for d in range(1, n_sp):
        devs.append((s + d < n_sp, (s + d, f, t)))
        devs.append((s - d >= 0, (s - d, f, t)))
    greet(devs)
    nxt = (s + 1, f, t)
    edge_copy = rcopy(edge, ed_out, g_send, g_recv, nxt)
    pl.when(s < n_sp - 1)(edge_copy.start)

    def pair(d):
        dev = (s + d, f, t)
        return (
            rcopy(state, st_out.at[d - 1], s_send.at[d - 1], s_recv.at[d - 1], dev),
            rcopy(decay, de_out.at[d - 1], c_send.at[d - 1], c_recv.at[d - 1], dev),
        )

    for d in range(1, n_sp):
        @pl.when(s + d < n_sp)
        def _():
            for c in pair(d):
                c.start()
    pl.when(s == 0)(lambda: ed_out.__setitem__(Ellipsis, jnp.zeros(ed_out.shape, ed_out.dtype)))
    for d in range(1, n_sp):
        @pl.when(s - d < 0)
        def _():
            st_out[d - 1] = jnp.zeros(st_out.shape[1:], st_out.dtype)
            de_out[d - 1] = jnp.ones(de_out.shape[1:], de_out.dtype)
    for d in range(1, n_sp):
        @pl.when(s - d >= 0)
        def _():
            for c in pair(d):
                c.wait_recv()
        @pl.when(s + d < n_sp)
        def _():
            for c in pair(d):
                c.wait_send()
    pl.when(s < n_sp - 1)(edge_copy.wait_send)
    pl.when(s > 0)(edge_copy.wait_recv)


def mix_kernel(
    n_sp, n_fs, n_tp, act, sq, ow, out,
    acts, sq_all, ow_all, relay_buf, wbuf, part,
    a_send, a_recv, f_send, d_send, d_recv, q_send, q_recv,
    up_send, down_send, o_recv, od_send, od_recv, m_send, m_recv,
):
    s, f, t = place()
    n_half = n_sp // n_tp
    rows = act.shape[1] // n_fs
    half = rows // n_tp
    width, cw = ow.shape[0] // 2, ow.shape[1]
    other = (s, f, 1 - t)
    px, py, pd = square(f)
    up, down = (s + 1, f, t), (s - 1, f, t)
    has_up, has_down = s < n_sp - 1, s > 0
    greet(
        [(None, other)]
        + [(None, (s, g, u)) for g in (px, py, pd) for u in (t, 1 - t)]
        + [(has_up, up), (has_down, down)]
    )

    def to_up(src, a):
        return rcopy(src, relay_buf.at[a], up_send.at[a], o_recv.at[a], up)

    def to_down(src, a):
        return rcopy(src, relay_buf.at[a], down_send.at[a], o_recv.at[a], down)

    def to_other(src, a):
        return rcopy(src, ow_all.at[lax.rem(a, n_half), t], od_send.at[a], od_recv.at[a], other)

    def keep(src, a):
        mine = a // n_half == t

        @pl.when(mine)
        def _():
            ow_all[lax.rem(a, n_half), t] = src[...]

        pl.when(jnp.logical_not(mine))(lambda: to_other(src, a).start())

    sends = []

    def send(c):
        c.start()
        sends.append(c)

    for i, (p, order) in enumerate(((px, (0, 1)), (py, (1, 0)))):
        for h in order:
            send(rcopy(act.at[h], acts.at[t, f, h], a_send.at[i, h], a_recv.at[f, h], (s, p, t)))
    pl.when(has_up)(lambda: to_up(ow, s).start())
    pl.when(has_down)(lambda: to_down(ow, s).start())
    for h in range(2):
        send(rcopy(act.at[h], acts.at[t, f, h], d_send.at[f, h], d_recv.at[f, h], other))
    for i, g in enumerate((px, py, pd)):
        for u in range(n_tp):
            send(rcopy(sq, sq_all.at[t, f], q_send.at[i, u], q_recv.at[t, f], (s, g, u)))
    send(rcopy(sq, sq_all.at[t, f], q_send.at[n_fs - 1, 0], q_recv.at[t, f], other))
    acts[t, f] = act[...]
    sq_all[t, f] = sq[...]
    keep(ow, s)

    def landed(g, h):
        here = acts.at[t, g, h]
        rcopy(here, here, d_send.at[g, h], a_recv.at[g, h], other).wait_recv()
        return here

    def hand_on(g, h, here):
        send(rcopy(here, here, d_send.at[g, h], d_recv.at[g, h], other))

    for i, (g, h, onto) in enumerate(((px, 0, py), (py, 1, px))):
        here = landed(g, h)
        send(rcopy(here, here, f_send.at[i], a_recv.at[g, h], (s, onto, t)))
        hand_on(g, h, here)

    def step(d):
        a = s - d

        @pl.when(a >= 0)
        def _():
            to_up(relay_buf.at[a], a).wait_recv()
            pl.when(has_up)(lambda: to_up(relay_buf.at[a], a).start())
            keep(relay_buf.at[a], a)
        b = s + d

        @pl.when(b < n_sp)
        def _():
            to_down(relay_buf.at[b], b).wait_recv()
            pl.when(has_down)(lambda: to_down(relay_buf.at[b], b).start())
            keep(relay_buf.at[b], b)

    for d in range(1, n_sp):
        step(d)
    for g, h in ((px, 1), (py, 0), (pd, 0), (pd, 1)):
        hand_on(g, h, landed(g, h))
    for i in range(n_half):
        a = t * n_half + i
        here = ow_all.at[i, 1 - t]
        rcopy(here, here, od_send.at[a], od_recv.at[a], other).wait_recv()
    for i in range(n_half):
        for u in range(n_tp):
            for k in range(2):
                wbuf[k, u * width : (u + 1) * width, i * cw : (i + 1) * cw] = ow_all[i, u, k * width : (k + 1) * width, :]
    for g in (px, py, pd):
        for u in range(n_tp):
            here = sq_all.at[u, g]
            rcopy(here, here, q_send.at[0, 0], q_recv.at[u, g], other).wait_recv()
    here = sq_all.at[1 - t, f]
    rcopy(here, here, q_send.at[0, 0], q_recv.at[1 - t, f], other).wait_recv()
    for g in (f, px, py, pd):
        for h in range(2):
            here = acts.at[1 - t, g, h]
            rcopy(here, here, d_send.at[g, h], d_recv.at[g, h], other).wait_recv()

    def piece(g, u):
        return rcopy(part.at[g, u], out.at[f, t], m_send.at[g, u], m_recv.at[f, t], (s, g, u))

    def spread(g):
        for u in range(n_tp):
            c = piece(g, u)
            c.start()
            sends.append(c)

    last = None
    for g in (pd, f, px, py):
        here = pl.ds(pl.multiple_of(g * rows, rows), rows)
        sums = sum(sq_all[u, i, g] for u in range(n_tp) for i in range(n_fs))
        scale = lax.rsqrt(sums / (n_tp * width) + EPS).T
        scale = jnp.concatenate([scale[:, i : i + 1] for i in range(rows // 128)], axis=0)
        left = [
            jnp.concatenate([acts[u, i, h, here, :] for u in range(n_tp) for i in range(n_fs)], axis=1)
            for h in range(2)
        ]
        mixed = (
            jnp.dot(left[0], wbuf[0], preferred_element_type=F32) * scale
            + jnp.dot(left[1], wbuf[1], preferred_element_type=F32)
        ).astype(BF)
        for u in range(n_tp):
            part[g, u] = mixed[u * half : (u + 1) * half]
        if last is not None and last is not f:
            spread(last)
        if last is f:
            c = piece(f, 1 - t)
            c.start()
            sends.append(c)
        last = g
    out[f, t] = part[f, t]
    for i in range(n_half):
        to_other(ow, (1 - t) * n_half + i).wait_send()
    for d in range(n_sp):
        a, b = s - d, s + d

        @pl.when((a >= 0) & has_up)
        def _():
            to_up(ow, a).wait_send()

        @pl.when((b < n_sp) & has_down)
        def _():
            to_down(ow, b).wait_send()
    spread(last)
    for c in sends:
        c.wait_send()
    for g in (px, py, pd):
        for u in range(n_tp):
            here = out.at[g, u]
            rcopy(here, here, m_send.at[g, u], m_recv.at[g, u], other).wait_recv()
    here = out.at[f, 1 - t]
    rcopy(here, here, m_send.at[f, 1 - t], m_recv.at[f, 1 - t], other).wait_recv()


def vmem(count):
    return [pl.BlockSpec(memory_space=pltpu.VMEM)] * count


def dma(*shape):
    return pltpu.SemaphoreType.DMA(shape) if shape else pltpu.SemaphoreType.DMA


def comm(kernel, outs, scratch, number, name):
    return pl.pallas_call(
        kernel,
        out_shape=[jax.ShapeDtypeStruct(a, b) for a, b in outs],
        out_specs=vmem(len(outs)),
        scratch_shapes=scratch,
        compiler_params=pltpu.CompilerParams(
            collective_id=number, has_side_effects=True, vmem_limit_bytes=60 * 1024 * 1024
        ),
        name=name,
    )


def local_recurrence(queries, input_gate, values, log_forget):
    tok_rows, head_count = (queries.shape[0], queries.shape[1])
    block_count = tok_rows // BLOCK
    q_blk, k_blk, v_blk, g_blk = (
        arr.reshape(block_count, BLOCK, head_count, HEAD_DIM)
        for arr in (queries, input_gate, values, log_forget)
    )
    within = jnp.cumsum(g_blk, axis=1)
    block_end = within[:, -1]
    q_up = q_blk * jnp.exp(within)
    k_down = k_blk * jnp.exp(-within)
    causal = jnp.tril(jnp.ones((BLOCK, BLOCK), jnp.bool_))
    scores = jnp.einsum("nthd,nshd->nhts", q_up, k_down, precision=HIGH)
    scores = jnp.where(causal, scores, 0.0)
    inner_out = jnp.einsum("nhts,nshe->nthe", scores, v_blk, precision=HIGH)
    updates = jnp.einsum(
        "nshd,nshe->nhde", k_blk * jnp.exp(block_end[:, None] - within), v_blk, precision=HIGH
    )
    decays = jnp.exp(block_end)
    state = jnp.zeros((head_count, HEAD_DIM, HEAD_DIM), F32)
    incoming = []
    for n in range(block_count):
        incoming.append(state)
        state = decays[n][:, :, None] * state + updates[n]
    offsets = jnp.cumsum(block_end, axis=0) - block_end
    total_log = jnp.sum(block_end, axis=0)
    return (inner_out, q_up, jnp.stack(incoming), jnp.exp(offsets), state, total_log)


def body(
    n_sp, n_fs, n_tp, tokens, norm_gain, w_query, forget_weight, w_input, w_outgate, w_pool, forget_gap,
    extra_decay, rec_gain, group_weight, pool_gain, recurrent_output_weight, w_out_pool,
):
    s, f, t = place()
    rows, half = tokens.shape[1:]
    width = w_query.shape[1]
    ch = width // n_fs
    n_w = 5
    wr = w_query.shape[0]
    lanes = rows // 128
    extra = jnp.pad(extra_decay[0].T.reshape(n_fs, lanes, 128), ((0, 0), (0, 8 - lanes), (0, 0)))
    cw = w_out_pool.shape[1]
    z, e_all, ow = comm(
        functools.partial(project_kernel, n_sp, n_fs, n_tp),
        [((n_fs, rows, n_w * ch), BF), ((n_fs, 8, 128), F32), ((2 * width, cw), BF)],
        [
            pltpu.VMEM((n_fs, wr, n_w * ch), BF), pltpu.VMEM((n_fs, rows, n_tp * half), BF),
            pltpu.VMEM((n_sp * n_fs * wr, n_w * ch), BF), pltpu.VMEM((n_fs, rows, n_w * ch), F32),
            dma(2, 2), dma(n_fs, 2), dma(2), dma(n_fs, 2), dma(n_fs, 2), dma(n_fs - 1), dma(n_sp, n_fs),
            dma(n_sp, n_fs), dma(n_sp, n_fs), dma(n_fs - 1), dma(n_fs),
        ],
        1, "project",
    )(
        tokens[0], w_query, forget_weight, w_input, w_outgate, w_pool, extra, norm_gain[None],
        group_weight, pool_gain[None], recurrent_output_weight, w_out_pool,
    )
    zf = z.astype(F32).transpose(1, 0, 2).reshape(rows, n_fs, n_w, ch)
    z_query, z_forget, z_input, z_outgate, z_pool = (zf[:, :, i] for i in range(n_w))
    gap = lax.dynamic_slice_in_dim(forget_gap, f * ch, ch, 0)
    gain = lax.dynamic_slice_in_dim(rec_gain, f * ch, ch, 0)
    decay_in = e_all[:, :lanes].reshape(n_fs, rows).T
    input_gate = gap * jax.nn.sigmoid(-z_forget)
    log_forget = jnp.log1p(-input_gate) + decay_in[:, :, None]
    inner_out, q_up, incoming, off, end_state, total_log = local_recurrence(
        jax.nn.silu(z_query), input_gate, z_input, log_forget
    )
    reach = 2**POOL_GROUPS
    tail = z[:, rows - reach :, (n_w - 1) * ch :]
    st, de, rim = comm(
        functools.partial(state_kernel, n_sp),
        [((n_sp - 1, n_fs, ch, ch), BF), ((n_sp - 1, n_fs, ch), F32), ((n_fs, reach, ch), BF)],
        [dma(n_sp - 1), dma(n_sp - 1), dma(n_sp - 1), dma(n_sp - 1), dma(), dma()],
        2, "state",
    )(end_state.astype(BF), jnp.exp(total_log), tail)
    total = jnp.zeros((n_fs, ch, ch), F32)
    for d in range(n_sp - 2, -1, -1):
        total = de[d][:, :, None] * total + st[d].astype(F32)
    entering = incoming + off[:, :, :, None] * total[None]
    recurrent = (inner_out + jnp.einsum("nthd,nhde->nthe", q_up, entering, precision=HIGH)).reshape(rows, n_fs, ch)
    square_sum = jnp.sum(recurrent * recurrent, axis=2)
    rec_act = (recurrent * gain * jax.nn.silu(z_outgate)).astype(BF).transpose(1, 0, 2).reshape(n_fs * rows, ch)
    sq = jnp.pad(square_sum.T.reshape(n_fs, lanes, 128), ((0, 0), (0, 8 - lanes), (0, 0)))

    zp = z[:, :, (n_w - 1) * ch :]
    running = jnp.concatenate([rim, zp], axis=1).astype(F32)
    group_dim = group_weight.shape[1]
    group = (t * width + f * ch) // group_dim
    window_total = None
    for level in range(POOL_GROUPS):
        stride = 2**level
        running = running[:, stride:] + running[:, :-stride]
        now = running[:, running.shape[1] - rows :]
        window_total = now if level == 0 else jnp.where(group == level, now, window_total)
    spot = s * rows + jnp.arange(rows, dtype=jnp.int32)
    counts = jnp.minimum(spot + 1, jnp.left_shift(jnp.int32(2), group)).astype(F32)
    pooled = (window_total / counts[None, :, None] - zp.astype(F32)).astype(BF).reshape(n_fs * rows, ch)

    n_half = n_sp // n_tp
    act = jnp.stack([rec_act, pooled])
    out_shape = (n_fs, n_tp, rows // n_tp, n_half * cw)
    (final,) = comm(
        functools.partial(mix_kernel, n_sp, n_fs, n_tp),
        [(out_shape, BF)],
        [
            pltpu.VMEM((n_tp, n_fs) + act.shape, BF), pltpu.VMEM((n_tp, n_fs) + sq.shape, F32),
            pltpu.VMEM((n_half, n_tp) + ow.shape, BF), pltpu.VMEM((n_sp,) + ow.shape, BF),
            pltpu.VMEM((2, n_tp * width, n_half * cw), BF), pltpu.VMEM(out_shape, BF),
            dma(2, 2), dma(n_fs, 2), dma(2), dma(n_fs, 2), dma(n_fs, 2), dma(n_fs, n_tp), dma(n_tp, n_fs),
            dma(n_sp), dma(n_sp), dma(n_sp), dma(n_sp), dma(n_sp), dma(n_fs, n_tp), dma(n_fs, n_tp),
        ],
        3, "mix",
    )(act, sq, ow)
    final = final.reshape(n_fs, n_tp, rows // n_tp, n_half, cw).transpose(2, 1, 3, 0, 4)
    return final.reshape(1, rows // n_tp, n_tp * n_half * n_fs * cw)


def solution(mesh):
    sizes = dict(mesh.shape)
    weight = P(("sp", "fs"), "tp")
    placed = (
        P("fs", "sp", "tp"), P(), weight, weight, weight, weight, weight, P("tp"),
        P("fs", "sp", "tp"), P("tp"), P(), P("tp"), P("tp", ("sp", "fs")), P("tp", ("sp", "fs")),
    )
    return jax.shard_map(
        functools.partial(body, sizes["sp"], sizes["fs"], sizes["tp"]),
        mesh=mesh, in_specs=placed, out_specs=P("fs", ("sp", "tp"), None), check_vma=False,
    )
```

```python
import functools
import jax
import jax.numpy as jnp
from jax import lax
from jax.experimental import pallas as pl
from jax.experimental.pallas import tpu as pltpu
from jax.sharding import PartitionSpec as P

HEAD_DIM = 128
POOL_GROUPS = 4
BLOCK = 64
EPS = 1e-06
HIGH = lax.Precision.HIGHEST
MESH = pl.DeviceIdType.MESH
BF = jnp.bfloat16
F32 = jnp.float32


def place():
    return lax.axis_index("sp"), lax.axis_index("fs"), lax.axis_index("tp")


def rcopy(src, dst, ssem, rsem, dev):
    return pltpu.make_async_remote_copy(
        src_ref=src, dst_ref=dst, send_sem=ssem, recv_sem=rsem, device_id=dev, device_id_type=MESH
    )


def greet(devs):
    barrier = pltpu.get_barrier_semaphore()
    for cond, dev in devs:
        def tell(dev=dev):
            pl.semaphore_signal(barrier, inc=1, device_id=dev, device_id_type=MESH)
        if cond is None:
            tell()
        else:
            pl.when(cond)(tell)
    pl.semaphore_wait(barrier, sum(1 if cond is None else jnp.where(cond, 1, 0) for cond, _ in devs))


def square(f):
    near = f + 1 - 2 * lax.rem(f, 2)
    return near, lax.rem(f + 2, 4), lax.rem(near + 2, 4)


def project_kernel(
    n_sp, n_fs, n_tp, tok, wq, wf, wi, wo, wp, extra, gain, gmap, pgain, wor, wop, z_ref, e_ref, ow_ref,
    wsrc, xs, ws, acc, x_send, x_recv, f_send, d_send, d_recv, w_send, w_recv, zr_send, zl_send, e_send, e_recv,
):
    s, f, t = place()
    rows, half = tok.shape
    part = rows // 2
    mats = (wq, wf, wi, wo, wp)
    wr, width = wq.shape
    ch = width // n_fs
    for i, w in enumerate(mats):
        for g in range(n_fs):
            wsrc[g, :, i * ch : (i + 1) * ch] = w[:, g * ch : (g + 1) * ch]
    other = (s, f, 1 - t)
    px, py, pd = square(f)
    order = (f, px, py, pd)
    up, down = (s + 1, f, t), (s - 1, f, t)
    has_up, has_down = s < n_sp - 1, s > 0
    greet([(None, other)] + [(None, (s, g, t)) for g in order[1:]] + [(has_up, up), (has_down, down)])

    def cols(c):
        return pl.ds(pl.multiple_of(c * half, half), half)

    def span(a, b):
        return pl.ds(pl.multiple_of((a * n_fs + b) * wr, wr), wr)

    def slot(a, b):
        return ws.at[span(a, b), :]

    def to_up(src, a, b):
        return rcopy(src, slot(a, b), zr_send.at[a, b], w_recv.at[a, b], up)

    def to_down(src, a, b):
        return rcopy(src, slot(a, b), zl_send.at[a, b], w_recv.at[a, b], down)

    sends = []

    def send(c):
        c.start()
        sends.append(c)

    def x_slot(g, h, c):
        return xs.at[g, h * part : (h + 1) * part, cols(c)]

    own = wsrc.at[f]
    pl.when(has_up)(lambda: to_up(own, s, f).start())
    pl.when(has_down)(lambda: to_down(own, s, f).start())
    for i, g in enumerate((pd, px, py)):
        send(rcopy(wsrc.at[g], slot(s, f), w_send.at[i], w_recv.at[s, f], (s, g, t)))
    for i, (p, hs) in enumerate(((px, (0, 1)), (py, (1, 0)))):
        for h in hs:
            send(rcopy(tok.at[h * part : (h + 1) * part, :], x_slot(f, h, t), x_send.at[i, h], x_recv.at[f, h], (s, p, t)))
    for h in range(2):
        send(rcopy(tok.at[h * part : (h + 1) * part, :], x_slot(f, h, t), d_send.at[f, h], d_recv.at[f, h], other))
    for i, g in enumerate(order[1:]):
        send(rcopy(extra.at[g], e_ref.at[f], e_send.at[i], e_recv.at[f], (s, g, t)))
    ws[span(s, f), :] = wsrc[f]
    xs[f, :, cols(t)] = tok[...]
    e_ref[f] = extra[f]
    ow_ref[0:width, :] = wor[...]
    gd = gmap.shape[1]
    for i in range(width // gd):
        at = slice(i * gd, (i + 1) * gd)
        scaled = (gmap[t * (width // gd) + i].astype(F32) * pgain[:, at]).astype(BF)
        folded = jnp.dot(scaled, wop[at, :], preferred_element_type=F32)
        ow_ref[width + i * gd : width + (i + 1) * gd, :] = folded.astype(BF)

    for g in order[1:]:
        to_up(slot(s, g), s, g).wait_recv()
        pl.when(has_up)(lambda: to_up(slot(s, g), s, g).start())
        pl.when(has_down)(lambda: to_down(slot(s, g), s, g).start())

    def landed(g, h):
        here = x_slot(g, h, t)
        rcopy(here, here, d_send.at[g, h], x_recv.at[g, h], other).wait_recv()
        return here

    def hand_on(g, h, here):
        send(rcopy(here, here, d_send.at[g, h], d_recv.at[g, h], other))

    for i, (g, h, onto) in enumerate(((px, 0, py), (py, 1, px))):
        here = landed(g, h)
        send(rcopy(here, here, f_send.at[i], x_recv.at[g, h], (s, onto, t)))
        hand_on(g, h, here)

    def relay(d):
        for g in order:
            a = s - d

            @pl.when(a >= 0)
            def _():
                to_up(slot(a, g), a, g).wait_recv()
                pl.when(has_up)(lambda: to_up(slot(a, g), a, g).start())
            b = s + d

            @pl.when(b < n_sp)
            def _():
                to_down(slot(b, g), b, g).wait_recv()
                pl.when(has_down)(lambda: to_down(slot(b, g), b, g).start())

    def add(a):
        k = pl.ds(pl.multiple_of(a * n_fs * wr, n_fs * wr), n_fs * wr)

        def each(i, _):
            acc[i] += jnp.dot(xs[i, :, k], ws[k, :], preferred_element_type=F32)
            return 0

        lax.fori_loop(0, n_fs, each, 0)

    def multiply(d):
        pl.when(s - d >= 0)(lambda: add(s - d))
        pl.when(s + d < n_sp)(lambda: add(s + d))

    relay(1)
    for g, h in ((px, 1), (py, 0), (pd, 0), (pd, 1)):
        hand_on(g, h, landed(g, h))
    for d in range(2, n_sp - 1):
        relay(d)
    for g in order:
        for h in range(2):
            here = x_slot(g, h, 1 - t)
            rcopy(here, here, d_send.at[g, h], d_recv.at[g, h], other).wait_recv()
    for g in order[1:]:
        rcopy(extra.at[f], e_ref.at[g], e_send.at[0], e_recv.at[g], other).wait_recv()
    for c in sends:
        c.wait_send()

    def norm(j, _):
        tile = 16
        per = rows // tile
        at = (j // per, pl.ds(pl.multiple_of(lax.rem(j, per) * tile, tile), tile))
        feats = xs[at[0], at[1], :].astype(F32)
        scale = lax.rsqrt(jnp.mean(feats * feats, axis=-1, keepdims=True) + EPS)
        xs[at[0], at[1], :] = (feats * scale * gain[...]).astype(BF)
        return 0

    lax.fori_loop(0, n_fs * rows // 16, norm, 0, unroll=2)

    if n_fs * wr % 128 == 0:
        own_k = pl.ds(pl.multiple_of(s * n_fs * wr, n_fs * wr), n_fs * wr)

        def begin(i, _):
            acc[i] = jnp.dot(xs[i, :, own_k], ws[own_k, :], preferred_element_type=F32)
            return 0

        lax.fori_loop(0, n_fs, begin, 0)
        for d in range(1, n_sp - 1):
            multiply(d)
        relay(n_sp - 1)
        multiply(n_sp - 1)

        def finish(i, _):
            z_ref[i] = acc[i].astype(BF)
            return 0
    else:
        relay(n_sp - 1)

        def finish(i, _):
            z_ref[i] = jnp.dot(xs[i], ws[...], preferred_element_type=F32).astype(BF)
            return 0

    lax.fori_loop(0, n_fs, finish, 0)

    for d in range(n_sp):
        for g in order:
            a = s - d

            @pl.when((a >= 0) & has_up)
            def _():
                to_up(slot(a, g), a, g).wait_send()
            b = s + d

            @pl.when((b < n_sp) & has_down)
            def _():
                to_down(slot(b, g), b, g).wait_send()


def dot(a, b, dims):
    return lax.dot_general(a, b, (dims, ((), ())), precision=HIGH, preferred_element_type=F32)


def state_kernel(
    n_sp, group_dim, z, e_all, gap, rec_gain, act, sq_out,
    local, qd, own_st, own_de, st_in, de_in, rim, s_send, s_recv, c_send, c_recv, g_send, g_recv,
):
    s, f, t = place()
    n_fs, rows, _ = z.shape
    ch = HEAD_DIM
    reach = rim.shape[1]
    devs = []
    for d in range(1, n_sp):
        devs.append((s + d < n_sp, (s + d, f, t)))
        devs.append((s - d >= 0, (s - d, f, t)))
    greet(devs)
    edge = rcopy(z.at[:, rows - reach :, 4 * ch :], rim, g_send, g_recv, (s + 1, f, t))
    pl.when(s < n_sp - 1)(edge.start)
    mine = pl.ds(pl.multiple_of(f * ch, ch), ch)
    gap_f = gap[:, mine]
    gain_f = rec_gain[:, mine]
    at = lax.broadcasted_iota(jnp.int32, (BLOCK, BLOCK), 0)
    causal = at >= lax.broadcasted_iota(jnp.int32, (BLOCK, BLOCK), 1)
    lower = causal.astype(F32)

    def one(g, _):
        state = jnp.zeros((ch, ch), F32)
        so_far = jnp.zeros((1, ch), F32)
        e_cols = e_all[g].T
        for n in range(rows // BLOCK):
            here = slice(n * BLOCK, (n + 1) * BLOCK)
            q, fo, v = (z[g, here, i * ch : (i + 1) * ch].astype(F32) for i in range(3))
            q = jax.nn.silu(q)
            k = gap_f * jax.nn.sigmoid(-fo)
            lo = n * BLOCK % 128
            lane = n * BLOCK // 128
            logs = jnp.log1p(-k) + e_cols[lo : lo + BLOCK, lane : lane + 1]
            within = dot(lower, logs, ((1,), (0,)))
            end = within[BLOCK - 1 :]
            q_up = q * jnp.exp(within)
            scores = jnp.where(causal, dot(q_up, k * jnp.exp(-within), ((1,), (1,))), 0.0)
            out = dot(scores, v, ((1,), (0,)))
            if n:
                out = out + dot(q_up, state, ((1,), (1,)))
            local[g, here, :] = out
            qd[g, here, :] = q_up * jnp.exp(so_far)
            state = state * jnp.exp(end) + dot(v.T, k * jnp.exp(end - within), ((1,), (0,)))
            so_far = so_far + end
        own_st[g] = state.astype(BF)
        own_de[g] = jnp.broadcast_to(jnp.exp(so_far), (8, ch))
        return 0

    lax.fori_loop(0, n_fs, one, 0)

    def pair(d):
        dev = (s + d, f, t)
        return (
            rcopy(own_st, st_in.at[d - 1], s_send.at[d - 1], s_recv.at[d - 1], dev),
            rcopy(own_de, de_in.at[d - 1], c_send.at[d - 1], c_recv.at[d - 1], dev),
        )

    for d in range(1, n_sp):
        @pl.when(s + d < n_sp)
        def _():
            for c in pair(d):
                c.start()

        @pl.when(s - d < 0)
        def _():
            st_in[d - 1] = jnp.zeros(st_in.shape[1:], st_in.dtype)
            de_in[d - 1] = jnp.ones(de_in.shape[1:], de_in.dtype)
    pl.when(s == 0)(lambda: rim.__setitem__(Ellipsis, jnp.zeros(rim.shape, rim.dtype)))
    pl.when(s > 0)(edge.wait_recv)
    group = (t * n_fs * ch + f * ch) // group_dim
    spot = s * rows + lax.broadcasted_iota(jnp.int32, (rows, ch), 0)
    window = 2
    for level in range(1, POOL_GROUPS):
        window = jnp.where(group == level, 2 ** (level + 1), window)
    counts = jnp.minimum(spot + 1, window).astype(F32)
    for g in range(n_fs):
        zp = z[g, :, 4 * ch :].astype(F32)
        running = jnp.concatenate([rim[g].astype(F32), zp], axis=0)
        total = None
        for level in range(POOL_GROUPS):
            stride = 2**level
            running = running[stride:] + running[:-stride]
            now = running[running.shape[0] - rows :]
            total = now if level == 0 else jnp.where(group == level, now, total)
        act[1, g * rows : (g + 1) * rows, :] = (total / counts - zp).astype(BF)
    for d in range(1, n_sp):
        @pl.when(s - d >= 0)
        def _():
            for c in pair(d):
                c.wait_recv()

    ones = jnp.ones((8, ch), F32)

    def finish(g, _):
        total = jnp.zeros((ch, ch), F32)
        for d in range(n_sp - 2, -1, -1):
            total = de_in[d, g, 0:1, :] * total + st_in[d, g].astype(F32)
        rec = local[g] + dot(qd[g], total, ((1,), (1,)))
        sums = dot(ones, rec * rec, ((1,), (1,)))
        for i in range(rows // 128):
            sq_out[g, i : i + 1, :] = sums[0:1, i * 128 : (i + 1) * 128]
        gate = jax.nn.silu(z[g, :, 3 * ch : 4 * ch].astype(F32))
        act[0, pl.ds(pl.multiple_of(g * rows, rows), rows), :] = (rec * gain_f * gate).astype(BF)
        return 0

    sq_out[...] = jnp.zeros(sq_out.shape, F32)
    lax.fori_loop(0, n_fs, finish, 0)
    for d in range(1, n_sp):
        @pl.when(s + d < n_sp)
        def _():
            for c in pair(d):
                c.wait_send()
    pl.when(s < n_sp - 1)(edge.wait_send)


def mix_kernel(
    n_sp, n_fs, n_tp, act, sq, ow, out,
    acts, sq_all, ow_all, relay_buf, wbuf, part,
    a_send, a_recv, f_send, d_send, d_recv, q_send, q_recv,
    up_send, down_send, o_recv, od_send, od_recv, m_send, m_recv,
):
    s, f, t = place()
    n_half = n_sp // n_tp
    rows = act.shape[1] // n_fs
    half = rows // n_tp
    width, cw = ow.shape[0] // 2, ow.shape[1]
    other = (s, f, 1 - t)
    px, py, pd = square(f)
    up, down = (s + 1, f, t), (s - 1, f, t)
    has_up, has_down = s < n_sp - 1, s > 0
    greet(
        [(None, other)]
        + [(None, (s, g, u)) for g in (px, py, pd) for u in (t, 1 - t)]
        + [(has_up, up), (has_down, down)]
    )

    def to_up(src, a):
        return rcopy(src, relay_buf.at[a], up_send.at[a], o_recv.at[a], up)

    def to_down(src, a):
        return rcopy(src, relay_buf.at[a], down_send.at[a], o_recv.at[a], down)

    def to_other(src, a):
        return rcopy(src, ow_all.at[lax.rem(a, n_half), t], od_send.at[a], od_recv.at[a], other)

    def keep(src, a):
        mine = a // n_half == t

        @pl.when(mine)
        def _():
            ow_all[lax.rem(a, n_half), t] = src[...]

        pl.when(jnp.logical_not(mine))(lambda: to_other(src, a).start())

    sends = []

    def send(c):
        c.start()
        sends.append(c)

    for i, (p, order) in enumerate(((px, (0, 1)), (py, (1, 0)))):
        for h in order:
            send(rcopy(act.at[h], acts.at[t, f, h], a_send.at[i, h], a_recv.at[f, h], (s, p, t)))
    pl.when(has_up)(lambda: to_up(ow, s).start())
    pl.when(has_down)(lambda: to_down(ow, s).start())
    for h in range(2):
        send(rcopy(act.at[h], acts.at[t, f, h], d_send.at[f, h], d_recv.at[f, h], other))
    for i, g in enumerate((px, py, pd)):
        for u in range(n_tp):
            send(rcopy(sq, sq_all.at[t, f], q_send.at[i, u], q_recv.at[t, f], (s, g, u)))
    send(rcopy(sq, sq_all.at[t, f], q_send.at[n_fs - 1, 0], q_recv.at[t, f], other))
    acts[t, f] = act[...]
    sq_all[t, f] = sq[...]
    keep(ow, s)

    def landed(g, h):
        here = acts.at[t, g, h]
        rcopy(here, here, d_send.at[g, h], a_recv.at[g, h], other).wait_recv()
        return here

    def hand_on(g, h, here):
        send(rcopy(here, here, d_send.at[g, h], d_recv.at[g, h], other))

    for i, (g, h, onto) in enumerate(((px, 0, py), (py, 1, px))):
        here = landed(g, h)
        send(rcopy(here, here, f_send.at[i], a_recv.at[g, h], (s, onto, t)))
        hand_on(g, h, here)

    def step(d):
        a = s - d

        @pl.when(a >= 0)
        def _():
            to_up(relay_buf.at[a], a).wait_recv()
            pl.when(has_up)(lambda: to_up(relay_buf.at[a], a).start())
            keep(relay_buf.at[a], a)
        b = s + d

        @pl.when(b < n_sp)
        def _():
            to_down(relay_buf.at[b], b).wait_recv()
            pl.when(has_down)(lambda: to_down(relay_buf.at[b], b).start())
            keep(relay_buf.at[b], b)

    for d in range(1, n_sp):
        step(d)
    for g, h in ((px, 1), (py, 0), (pd, 0), (pd, 1)):
        hand_on(g, h, landed(g, h))
    for i in range(n_half):
        a = t * n_half + i
        here = ow_all.at[i, 1 - t]
        rcopy(here, here, od_send.at[a], od_recv.at[a], other).wait_recv()
    for i in range(n_half):
        for u in range(n_tp):
            for k in range(2):
                wbuf[k, u * width : (u + 1) * width, i * cw : (i + 1) * cw] = ow_all[i, u, k * width : (k + 1) * width, :]
    for g in (px, py, pd):
        for u in range(n_tp):
            here = sq_all.at[u, g]
            rcopy(here, here, q_send.at[0, 0], q_recv.at[u, g], other).wait_recv()
    here = sq_all.at[1 - t, f]
    rcopy(here, here, q_send.at[0, 0], q_recv.at[1 - t, f], other).wait_recv()
    for g in (f, px, py, pd):
        for h in range(2):
            here = acts.at[1 - t, g, h]
            rcopy(here, here, d_send.at[g, h], d_recv.at[g, h], other).wait_recv()

    def piece(g, u):
        return rcopy(part.at[g, u], out.at[f, t], m_send.at[g, u], m_recv.at[f, t], (s, g, u))

    def spread(g):
        for u in range(n_tp):
            c = piece(g, u)
            c.start()
            sends.append(c)

    last = None
    for g in (pd, f, px, py):
        here = pl.ds(pl.multiple_of(g * rows, rows), rows)
        sums = sum(sq_all[u, i, g] for u in range(n_tp) for i in range(n_fs))
        scale = lax.rsqrt(sums / (n_tp * width) + EPS).T
        scale = jnp.concatenate([scale[:, i : i + 1] for i in range(rows // 128)], axis=0)
        left = [
            jnp.concatenate([acts[u, i, h, here, :] for u in range(n_tp) for i in range(n_fs)], axis=1)
            for h in range(2)
        ]
        mixed = (
            jnp.dot(left[0], wbuf[0], preferred_element_type=F32) * scale
            + jnp.dot(left[1], wbuf[1], preferred_element_type=F32)
        ).astype(BF)
        for u in range(n_tp):
            part[g, u] = mixed[u * half : (u + 1) * half]
        if last is not None and last is not f:
            spread(last)
        if last is f:
            c = piece(f, 1 - t)
            c.start()
            sends.append(c)
        last = g
    out[f, t] = part[f, t]
    for i in range(n_half):
        to_other(ow, (1 - t) * n_half + i).wait_send()
    for d in range(n_sp):
        a, b = s - d, s + d

        @pl.when((a >= 0) & has_up)
        def _():
            to_up(ow, a).wait_send()

        @pl.when((b < n_sp) & has_down)
        def _():
            to_down(ow, b).wait_send()
    spread(last)
    for c in sends:
        c.wait_send()
    for g in (px, py, pd):
        for u in range(n_tp):
            here = out.at[g, u]
            rcopy(here, here, m_send.at[g, u], m_recv.at[g, u], other).wait_recv()
    here = out.at[f, 1 - t]
    rcopy(here, here, m_send.at[f, 1 - t], m_recv.at[f, 1 - t], other).wait_recv()


def vmem(count):
    return [pl.BlockSpec(memory_space=pltpu.VMEM)] * count


def dma(*shape):
    return pltpu.SemaphoreType.DMA(shape) if shape else pltpu.SemaphoreType.DMA


def comm(kernel, outs, scratch, number, name):
    return pl.pallas_call(
        kernel,
        out_shape=[jax.ShapeDtypeStruct(a, b) for a, b in outs],
        out_specs=vmem(len(outs)),
        scratch_shapes=scratch,
        compiler_params=pltpu.CompilerParams(
            collective_id=number, has_side_effects=True, vmem_limit_bytes=60 * 1024 * 1024
        ),
        name=name,
    )


def body(
    n_sp, n_fs, n_tp, tokens, norm_gain, w_query, forget_weight, w_input, w_outgate, w_pool, forget_gap,
    extra_decay, rec_gain, group_weight, pool_gain, recurrent_output_weight, w_out_pool,
):
    s, f, t = place()
    rows, half = tokens.shape[1:]
    width = w_query.shape[1]
    ch = width // n_fs
    n_w = 5
    wr = w_query.shape[0]
    lanes = rows // 128
    extra = jnp.pad(extra_decay[0].T.reshape(n_fs, lanes, 128), ((0, 0), (0, 8 - lanes), (0, 0)))
    cw = w_out_pool.shape[1]
    z, e_all, ow = comm(
        functools.partial(project_kernel, n_sp, n_fs, n_tp),
        [((n_fs, rows, n_w * ch), BF), ((n_fs, 8, 128), F32), ((2 * width, cw), BF)],
        [
            pltpu.VMEM((n_fs, wr, n_w * ch), BF), pltpu.VMEM((n_fs, rows, n_tp * half), BF),
            pltpu.VMEM((n_sp * n_fs * wr, n_w * ch), BF), pltpu.VMEM((n_fs, rows, n_w * ch), F32),
            dma(2, 2), dma(n_fs, 2), dma(2), dma(n_fs, 2), dma(n_fs, 2), dma(n_fs - 1), dma(n_sp, n_fs),
            dma(n_sp, n_fs), dma(n_sp, n_fs), dma(n_fs - 1), dma(n_fs),
        ],
        1, "project",
    )(
        tokens[0], w_query, forget_weight, w_input, w_outgate, w_pool, extra, norm_gain[None],
        group_weight, pool_gain[None], recurrent_output_weight, w_out_pool,
    )
    n_half = n_sp // n_tp
    act, sq = comm(
        functools.partial(state_kernel, n_sp, group_weight.shape[1]),
        [((2, n_fs * rows, ch), BF), ((n_fs, 8, 128), F32)],
        [
            pltpu.VMEM((n_fs, rows, ch), F32), pltpu.VMEM((n_fs, rows, ch), F32),
            pltpu.VMEM((n_fs, ch, ch), BF), pltpu.VMEM((n_fs, 8, ch), F32),
            pltpu.VMEM((n_sp - 1, n_fs, ch, ch), BF), pltpu.VMEM((n_sp - 1, n_fs, 8, ch), F32),
            pltpu.VMEM((n_fs, 2**POOL_GROUPS, ch), BF),
            dma(n_sp - 1), dma(n_sp - 1), dma(n_sp - 1), dma(n_sp - 1), dma(), dma(),
        ],
        2, "state",
    )(z, e_all, forget_gap[None], rec_gain[None])
    out_shape = (n_fs, n_tp, rows // n_tp, n_half * cw)
    (final,) = comm(
        functools.partial(mix_kernel, n_sp, n_fs, n_tp),
        [(out_shape, BF)],
        [
            pltpu.VMEM((n_tp, n_fs) + act.shape, BF), pltpu.VMEM((n_tp, n_fs) + sq.shape, F32),
            pltpu.VMEM((n_half, n_tp) + ow.shape, BF), pltpu.VMEM((n_sp,) + ow.shape, BF),
            pltpu.VMEM((2, n_tp * width, n_half * cw), BF), pltpu.VMEM(out_shape, BF),
            dma(2, 2), dma(n_fs, 2), dma(2), dma(n_fs, 2), dma(n_fs, 2), dma(n_fs, n_tp), dma(n_tp, n_fs),
            dma(n_sp), dma(n_sp), dma(n_sp), dma(n_sp), dma(n_sp), dma(n_fs, n_tp), dma(n_fs, n_tp),
        ],
        3, "mix",
    )(act, sq, ow)
    final = final.reshape(n_fs, n_tp, rows // n_tp, n_half, cw).transpose(2, 1, 3, 0, 4)
    return final.reshape(1, rows // n_tp, n_tp * n_half * n_fs * cw)


def solution(mesh):
    sizes = dict(mesh.shape)
    weight = P(("sp", "fs"), "tp")
    placed = (
        P("fs", "sp", "tp"), P(), weight, weight, weight, weight, weight, P("tp"),
        P("fs", "sp", "tp"), P("tp"), P(), P("tp"), P("tp", ("sp", "fs")), P("tp", ("sp", "fs")),
    )
    return jax.shard_map(
        functools.partial(body, sizes["sp"], sizes["fs"], sizes["tp"]),
        mesh=mesh, in_specs=placed, out_specs=P("fs", ("sp", "tp"), None), check_vma=False,
    )
```

```python
import functools
import jax
import jax.numpy as jnp
from jax import lax
from jax.experimental import pallas as pl
from jax.experimental.pallas import tpu as pltpu
from jax.sharding import PartitionSpec as P

HEAD_DIM = 128
POOL_GROUPS = 4
BLOCK = 64
EPS = 1e-06
HIGH = lax.Precision.HIGHEST
MESH = pl.DeviceIdType.MESH
BF = jnp.bfloat16
F32 = jnp.float32


def place():
    return lax.axis_index("sp"), lax.axis_index("fs"), lax.axis_index("tp")


def rcopy(src, dst, ssem, rsem, dev):
    return pltpu.make_async_remote_copy(
        src_ref=src, dst_ref=dst, send_sem=ssem, recv_sem=rsem, device_id=dev, device_id_type=MESH
    )


def greet(devs):
    barrier = pltpu.get_barrier_semaphore()
    for cond, dev in devs:
        def tell(dev=dev):
            pl.semaphore_signal(barrier, inc=1, device_id=dev, device_id_type=MESH)
        if cond is None:
            tell()
        else:
            pl.when(cond)(tell)
    pl.semaphore_wait(barrier, sum(1 if cond is None else jnp.where(cond, 1, 0) for cond, _ in devs))


def square(f):
    near = f + 1 - 2 * lax.rem(f, 2)
    return near, lax.rem(f + 2, 4), lax.rem(near + 2, 4)


def project_kernel(
    n_sp, n_fs, n_tp, tok, wq, wf, wi, wo, wp, extra, gain, gmap, pgain, wor, wop, z_ref, e_ref, ow_ref,
    wsrc, xs, ws, acc, x_send, x_recv, f_send, d_send, d_recv, w_send, w_recv, zr_send, zl_send, e_send, e_recv,
):
    s, f, t = place()
    rows, half = tok.shape
    part = rows // 2
    mats = (wq, wf, wi, wo, wp)
    wr, width = wq.shape
    ch = width // n_fs
    for i, w in enumerate(mats):
        for g in range(n_fs):
            wsrc[g, :, i * ch : (i + 1) * ch] = w[:, g * ch : (g + 1) * ch]
    other = (s, f, 1 - t)
    px, py, pd = square(f)
    order = (f, px, py, pd)
    up, down = (s + 1, f, t), (s - 1, f, t)
    has_up, has_down = s < n_sp - 1, s > 0
    greet([(None, other)] + [(None, (s, g, t)) for g in order[1:]] + [(has_up, up), (has_down, down)])

    def cols(c):
        return pl.ds(pl.multiple_of(c * half, half), half)

    def span(a, b):
        return pl.ds(pl.multiple_of((a * n_fs + b) * wr, wr), wr)

    def slot(a, b):
        return ws.at[span(a, b), :]

    def to_up(src, a, b):
        return rcopy(src, slot(a, b), zr_send.at[a, b], w_recv.at[a, b], up)

    def to_down(src, a, b):
        return rcopy(src, slot(a, b), zl_send.at[a, b], w_recv.at[a, b], down)

    sends = []

    def send(c):
        c.start()
        sends.append(c)

    def x_slot(g, h, c):
        return xs.at[g, h * part : (h + 1) * part, cols(c)]

    own = wsrc.at[f]
    pl.when(has_up)(lambda: to_up(own, s, f).start())
    pl.when(has_down)(lambda: to_down(own, s, f).start())
    for i, g in enumerate((pd, px, py)):
        send(rcopy(wsrc.at[g], slot(s, f), w_send.at[i], w_recv.at[s, f], (s, g, t)))
    for i, (p, hs) in enumerate(((px, (0, 1)), (py, (1, 0)))):
        for h in hs:
            send(rcopy(tok.at[h * part : (h + 1) * part, :], x_slot(f, h, t), x_send.at[i, h], x_recv.at[f, h], (s, p, t)))
    for h in range(2):
        send(rcopy(tok.at[h * part : (h + 1) * part, :], x_slot(f, h, t), d_send.at[f, h], d_recv.at[f, h], other))
    for i, g in enumerate(order[1:]):
        send(rcopy(extra.at[g], e_ref.at[f], e_send.at[i], e_recv.at[f], (s, g, t)))
    ws[span(s, f), :] = wsrc[f]
    xs[f, :, cols(t)] = tok[...]
    e_ref[f] = extra[f]
    ow_ref[0:width, :] = wor[...]
    gd = gmap.shape[1]
    for i in range(width // gd):
        at = slice(i * gd, (i + 1) * gd)
        scaled = (gmap[t * (width // gd) + i].astype(F32) * pgain[:, at]).astype(BF)
        folded = jnp.dot(scaled, wop[at, :], preferred_element_type=F32)
        ow_ref[width + i * gd : width + (i + 1) * gd, :] = folded.astype(BF)

    for g in order[1:]:
        to_up(slot(s, g), s, g).wait_recv()
        pl.when(has_up)(lambda: to_up(slot(s, g), s, g).start())
        pl.when(has_down)(lambda: to_down(slot(s, g), s, g).start())

    def landed(g, h):
        here = x_slot(g, h, t)
        rcopy(here, here, d_send.at[g, h], x_recv.at[g, h], other).wait_recv()
        return here

    def hand_on(g, h, here):
        send(rcopy(here, here, d_send.at[g, h], d_recv.at[g, h], other))

    for i, (g, h, onto) in enumerate(((px, 0, py), (py, 1, px))):
        here = landed(g, h)
        send(rcopy(here, here, f_send.at[i], x_recv.at[g, h], (s, onto, t)))
        hand_on(g, h, here)

    def relay(d):
        for g in order:
            a = s - d

            @pl.when(a >= 0)
            def _():
                to_up(slot(a, g), a, g).wait_recv()
                pl.when(has_up)(lambda: to_up(slot(a, g), a, g).start())
            b = s + d

            @pl.when(b < n_sp)
            def _():
                to_down(slot(b, g), b, g).wait_recv()
                pl.when(has_down)(lambda: to_down(slot(b, g), b, g).start())

    def add(a):
        k = pl.ds(pl.multiple_of(a * n_fs * wr, n_fs * wr), n_fs * wr)

        def each(i, _):
            acc[i] += jnp.dot(xs[i, :, k], ws[k, :], preferred_element_type=F32)
            return 0

        lax.fori_loop(0, n_fs, each, 0)

    def multiply(d):
        pl.when(s - d >= 0)(lambda: add(s - d))
        pl.when(s + d < n_sp)(lambda: add(s + d))

    relay(1)
    for g, h in ((px, 1), (py, 0), (pd, 0), (pd, 1)):
        hand_on(g, h, landed(g, h))
    for d in range(2, n_sp - 1):
        relay(d)
    for g in order:
        for h in range(2):
            here = x_slot(g, h, 1 - t)
            rcopy(here, here, d_send.at[g, h], d_recv.at[g, h], other).wait_recv()
    for g in order[1:]:
        rcopy(extra.at[f], e_ref.at[g], e_send.at[0], e_recv.at[g], other).wait_recv()
    for c in sends:
        c.wait_send()

    def norm(j, _):
        tile = 16
        per = rows // tile
        at = (j // per, pl.ds(pl.multiple_of(lax.rem(j, per) * tile, tile), tile))
        feats = xs[at[0], at[1], :].astype(F32)
        scale = lax.rsqrt(jnp.mean(feats * feats, axis=-1, keepdims=True) + EPS)
        xs[at[0], at[1], :] = (feats * scale * gain[...]).astype(BF)
        return 0

    lax.fori_loop(0, n_fs * rows // 16, norm, 0, unroll=2)

    if n_fs * wr % 128 == 0:
        own_k = pl.ds(pl.multiple_of(s * n_fs * wr, n_fs * wr), n_fs * wr)

        def begin(i, _):
            acc[i] = jnp.dot(xs[i, :, own_k], ws[own_k, :], preferred_element_type=F32)
            return 0

        lax.fori_loop(0, n_fs, begin, 0)
        for d in range(1, n_sp - 1):
            multiply(d)
        relay(n_sp - 1)
        multiply(n_sp - 1)

        def finish(i, _):
            z_ref[i] = acc[i].astype(BF)
            return 0
    else:
        relay(n_sp - 1)

        def finish(i, _):
            z_ref[i] = jnp.dot(xs[i], ws[...], preferred_element_type=F32).astype(BF)
            return 0

    lax.fori_loop(0, n_fs, finish, 0)

    for d in range(n_sp):
        for g in order:
            a = s - d

            @pl.when((a >= 0) & has_up)
            def _():
                to_up(slot(a, g), a, g).wait_send()
            b = s + d

            @pl.when((b < n_sp) & has_down)
            def _():
                to_down(slot(b, g), b, g).wait_send()


def dot(a, b, dims):
    return lax.dot_general(a, b, (dims, ((), ())), precision=HIGH, preferred_element_type=F32)


def state_kernel(
    n_sp, group_dim, z, e_all, gap, rec_gain, act, sq_out,
    local, qd, own_st, own_de, st_in, de_in, rim, s_send, s_recv, c_send, c_recv, g_send, g_recv,
):
    s, f, t = place()
    n_fs, rows, _ = z.shape
    ch = HEAD_DIM
    reach = rim.shape[1]
    devs = []
    for d in range(1, n_sp):
        devs.append((s + d < n_sp, (s + d, f, t)))
        devs.append((s - d >= 0, (s - d, f, t)))
    greet(devs)
    edge = rcopy(z.at[:, rows - reach :, 4 * ch :], rim, g_send, g_recv, (s + 1, f, t))
    pl.when(s < n_sp - 1)(edge.start)
    mine = pl.ds(pl.multiple_of(f * ch, ch), ch)
    gap_f = gap[:, mine]
    gain_f = rec_gain[:, mine]
    at = lax.broadcasted_iota(jnp.int32, (BLOCK, BLOCK), 0)
    causal = at >= lax.broadcasted_iota(jnp.int32, (BLOCK, BLOCK), 1)
    lower = causal.astype(F32)

    def one(g, _):
        state = jnp.zeros((ch, ch), F32)
        so_far = jnp.zeros((1, ch), F32)
        e_cols = e_all[g].T
        for n in range(rows // BLOCK):
            here = slice(n * BLOCK, (n + 1) * BLOCK)
            q, fo, v = (z[g, here, i * ch : (i + 1) * ch].astype(F32) for i in range(3))
            q = jax.nn.silu(q)
            k = gap_f * jax.nn.sigmoid(-fo)
            lo = n * BLOCK % 128
            lane = n * BLOCK // 128
            logs = jnp.log1p(-k) + e_cols[lo : lo + BLOCK, lane : lane + 1]
            within = dot(lower, logs, ((1,), (0,)))
            end = within[BLOCK - 1 :]
            q_up = q * jnp.exp(within)
            scores = jnp.where(causal, dot(q_up, k * jnp.exp(-within), ((1,), (1,))), 0.0)
            out = dot(scores, v, ((1,), (0,)))
            if n:
                out = out + dot(q_up, state, ((1,), (1,)))
            local[g, here, :] = out
            qd[g, here, :] = q_up * jnp.exp(so_far)
            state = state * jnp.exp(end) + dot(v.T, k * jnp.exp(end - within), ((1,), (0,)))
            so_far = so_far + end
        own_st[g] = state.astype(BF)
        own_de[g] = jnp.broadcast_to(jnp.exp(so_far), (8, ch))
        return 0

    lax.fori_loop(0, n_fs, one, 0)

    def pair(d):
        dev = (s + d, f, t)
        return (
            rcopy(own_st, st_in.at[d - 1], s_send.at[d - 1], s_recv.at[d - 1], dev),
            rcopy(own_de, de_in.at[d - 1], c_send.at[d - 1], c_recv.at[d - 1], dev),
        )

    for d in range(1, n_sp):
        @pl.when(s + d < n_sp)
        def _():
            for c in pair(d):
                c.start()

        @pl.when(s - d < 0)
        def _():
            st_in[d - 1] = jnp.zeros(st_in.shape[1:], st_in.dtype)
            de_in[d - 1] = jnp.ones(de_in.shape[1:], de_in.dtype)
    pl.when(s == 0)(lambda: rim.__setitem__(Ellipsis, jnp.zeros(rim.shape, rim.dtype)))
    pl.when(s > 0)(edge.wait_recv)
    group = (t * n_fs * ch + f * ch) // group_dim
    spot = s * rows + lax.broadcasted_iota(jnp.int32, (rows, ch), 0)
    window = 2
    for level in range(1, POOL_GROUPS):
        window = jnp.where(group == level, 2 ** (level + 1), window)
    counts = jnp.minimum(spot + 1, window).astype(F32)
    for g in range(n_fs):
        zp = z[g, :, 4 * ch :].astype(F32)
        running = jnp.concatenate([rim[g].astype(F32), zp], axis=0)
        total = None
        for level in range(POOL_GROUPS):
            stride = 2**level
            running = running[stride:] + running[:-stride]
            now = running[running.shape[0] - rows :]
            total = now if level == 0 else jnp.where(group == level, now, total)
        act[1, g * rows : (g + 1) * rows, :] = (total / counts - zp).astype(BF)
    for d in range(1, n_sp):
        @pl.when(s - d >= 0)
        def _():
            for c in pair(d):
                c.wait_recv()

    ones = jnp.ones((8, ch), F32)

    def finish(g, _):
        total = jnp.zeros((ch, ch), F32)
        for d in range(n_sp - 2, -1, -1):
            total = de_in[d, g, 0:1, :] * total + st_in[d, g].astype(F32)
        rec = local[g] + dot(qd[g], total, ((1,), (1,)))
        sums = dot(ones, rec * rec, ((1,), (1,)))
        for i in range(rows // 128):
            sq_out[g, i : i + 1, :] = sums[0:1, i * 128 : (i + 1) * 128]
        gate = jax.nn.silu(z[g, :, 3 * ch : 4 * ch].astype(F32))
        act[0, pl.ds(pl.multiple_of(g * rows, rows), rows), :] = (rec * gain_f * gate).astype(BF)
        return 0

    sq_out[...] = jnp.zeros(sq_out.shape, F32)
    lax.fori_loop(0, n_fs, finish, 0)
    for d in range(1, n_sp):
        @pl.when(s + d < n_sp)
        def _():
            for c in pair(d):
                c.wait_send()
    pl.when(s < n_sp - 1)(edge.wait_send)


def mix_kernel(
    n_sp, n_fs, n_tp, act, sq, ow, final,
    out, acts, sq_all, ow_all, relay_buf, wbuf, part,
    a_send, a_recv, f_send, d_send, d_recv, q_send, q_recv,
    up_send, down_send, o_recv, od_send, od_recv, m_send, m_recv,
):
    s, f, t = place()
    n_half = n_sp // n_tp
    rows = act.shape[1] // n_fs
    half = rows // n_tp
    width, cw = ow.shape[0] // 2, ow.shape[1]
    other = (s, f, 1 - t)
    px, py, pd = square(f)
    up, down = (s + 1, f, t), (s - 1, f, t)
    has_up, has_down = s < n_sp - 1, s > 0
    greet(
        [(None, other)]
        + [(None, (s, g, u)) for g in (px, py, pd) for u in (t, 1 - t)]
        + [(has_up, up), (has_down, down)]
    )

    def to_up(src, a):
        return rcopy(src, relay_buf.at[a], up_send.at[a], o_recv.at[a], up)

    def to_down(src, a):
        return rcopy(src, relay_buf.at[a], down_send.at[a], o_recv.at[a], down)

    def to_other(src, a):
        return rcopy(src, ow_all.at[lax.rem(a, n_half), t], od_send.at[a], od_recv.at[a], other)

    def keep(src, a):
        mine = a // n_half == t

        @pl.when(mine)
        def _():
            ow_all[lax.rem(a, n_half), t] = src[...]

        pl.when(jnp.logical_not(mine))(lambda: to_other(src, a).start())

    sends = []

    def send(c):
        c.start()
        sends.append(c)

    for i, (p, order) in enumerate(((px, (0, 1)), (py, (1, 0)))):
        for h in order:
            send(rcopy(act.at[h], acts.at[t, f, h], a_send.at[i, h], a_recv.at[f, h], (s, p, t)))
    pl.when(has_up)(lambda: to_up(ow, s).start())
    pl.when(has_down)(lambda: to_down(ow, s).start())
    for h in range(2):
        send(rcopy(act.at[h], acts.at[t, f, h], d_send.at[f, h], d_recv.at[f, h], other))
    for i, g in enumerate((px, py, pd)):
        for u in range(n_tp):
            send(rcopy(sq, sq_all.at[t, f], q_send.at[i, u], q_recv.at[t, f], (s, g, u)))
    send(rcopy(sq, sq_all.at[t, f], q_send.at[n_fs - 1, 0], q_recv.at[t, f], other))
    acts[t, f] = act[...]
    sq_all[t, f] = sq[...]
    keep(ow, s)

    def landed(g, h):
        here = acts.at[t, g, h]
        rcopy(here, here, d_send.at[g, h], a_recv.at[g, h], other).wait_recv()
        return here

    def hand_on(g, h, here):
        send(rcopy(here, here, d_send.at[g, h], d_recv.at[g, h], other))

    for i, (g, h, onto) in enumerate(((px, 0, py), (py, 1, px))):
        here = landed(g, h)
        send(rcopy(here, here, f_send.at[i], a_recv.at[g, h], (s, onto, t)))
        hand_on(g, h, here)

    def step(d):
        a = s - d

        @pl.when(a >= 0)
        def _():
            to_up(relay_buf.at[a], a).wait_recv()
            pl.when(has_up)(lambda: to_up(relay_buf.at[a], a).start())
            keep(relay_buf.at[a], a)
        b = s + d

        @pl.when(b < n_sp)
        def _():
            to_down(relay_buf.at[b], b).wait_recv()
            pl.when(has_down)(lambda: to_down(relay_buf.at[b], b).start())
            keep(relay_buf.at[b], b)

    for d in range(1, n_sp):
        step(d)
    for g, h in ((px, 1), (py, 0), (pd, 0), (pd, 1)):
        hand_on(g, h, landed(g, h))
    for i in range(n_half):
        a = t * n_half + i
        here = ow_all.at[i, 1 - t]
        rcopy(here, here, od_send.at[a], od_recv.at[a], other).wait_recv()
    for i in range(n_half):
        for u in range(n_tp):
            for k in range(2):
                wbuf[k, u * width : (u + 1) * width, i * cw : (i + 1) * cw] = ow_all[i, u, k * width : (k + 1) * width, :]
    for g in (px, py, pd):
        for u in range(n_tp):
            here = sq_all.at[u, g]
            rcopy(here, here, q_send.at[0, 0], q_recv.at[u, g], other).wait_recv()
    here = sq_all.at[1 - t, f]
    rcopy(here, here, q_send.at[0, 0], q_recv.at[1 - t, f], other).wait_recv()
    for g in (f, px, py, pd):
        for h in range(2):
            here = acts.at[1 - t, g, h]
            rcopy(here, here, d_send.at[g, h], d_recv.at[g, h], other).wait_recv()

    def piece(g, u):
        return rcopy(part.at[g, u], out.at[f, t], m_send.at[g, u], m_recv.at[f, t], (s, g, u))

    def spread(g):
        for u in range(n_tp):
            c = piece(g, u)
            c.start()
            sends.append(c)

    last = None
    for g in (pd, f, px, py):
        here = pl.ds(pl.multiple_of(g * rows, rows), rows)
        sums = sum(sq_all[u, i, g] for u in range(n_tp) for i in range(n_fs))
        scale = lax.rsqrt(sums / (n_tp * width) + EPS).T
        scale = jnp.concatenate([scale[:, i : i + 1] for i in range(rows // 128)], axis=0)
        left = [
            jnp.concatenate([acts[u, i, h, here, :] for u in range(n_tp) for i in range(n_fs)], axis=1)
            for h in range(2)
        ]
        mixed = (
            jnp.dot(left[0], wbuf[0], preferred_element_type=F32) * scale
            + jnp.dot(left[1], wbuf[1], preferred_element_type=F32)
        ).astype(BF)
        for u in range(n_tp):
            part[g, u] = mixed[u * half : (u + 1) * half]
        if last is not None and last is not f:
            spread(last)
        if last is f:
            c = piece(f, 1 - t)
            c.start()
            sends.append(c)
        last = g
    out[f, t] = part[f, t]
    for i in range(n_half):
        to_other(ow, (1 - t) * n_half + i).wait_send()
    for d in range(n_sp):
        a, b = s - d, s + d

        @pl.when((a >= 0) & has_up)
        def _():
            to_up(ow, a).wait_send()

        @pl.when((b < n_sp) & has_down)
        def _():
            to_down(ow, b).wait_send()
    spread(last)
    for c in sends:
        c.wait_send()
    for g in (px, py, pd):
        for u in range(n_tp):
            here = out.at[g, u]
            rcopy(here, here, m_send.at[g, u], m_recv.at[g, u], other).wait_recv()
    here = out.at[f, 1 - t]
    rcopy(here, here, m_send.at[f, 1 - t], m_recv.at[f, 1 - t], other).wait_recv()
    for u in range(n_tp):
        for i in range(n_half):
            for g in range(n_fs):
                lo = ((u * n_half + i) * n_fs + g) * cw
                final[:, lo : lo + cw] = out[g, u, :, i * cw : (i + 1) * cw]


def vmem(count):
    return [pl.BlockSpec(memory_space=pltpu.VMEM)] * count


def dma(*shape):
    return pltpu.SemaphoreType.DMA(shape) if shape else pltpu.SemaphoreType.DMA


def comm(kernel, outs, scratch, number, name):
    return pl.pallas_call(
        kernel,
        out_shape=[jax.ShapeDtypeStruct(a, b) for a, b in outs],
        out_specs=vmem(len(outs)),
        scratch_shapes=scratch,
        compiler_params=pltpu.CompilerParams(
            collective_id=number, has_side_effects=True, vmem_limit_bytes=60 * 1024 * 1024
        ),
        name=name,
    )


def body(
    n_sp, n_fs, n_tp, tokens, norm_gain, w_query, forget_weight, w_input, w_outgate, w_pool, forget_gap,
    extra_decay, rec_gain, group_weight, pool_gain, recurrent_output_weight, w_out_pool,
):
    s, f, t = place()
    rows, half = tokens.shape[1:]
    width = w_query.shape[1]
    ch = width // n_fs
    n_w = 5
    wr = w_query.shape[0]
    lanes = rows // 128
    extra = jnp.pad(extra_decay[0].T.reshape(n_fs, lanes, 128), ((0, 0), (0, 8 - lanes), (0, 0)))
    cw = w_out_pool.shape[1]
    z, e_all, ow = comm(
        functools.partial(project_kernel, n_sp, n_fs, n_tp),
        [((n_fs, rows, n_w * ch), BF), ((n_fs, 8, 128), F32), ((2 * width, cw), BF)],
        [
            pltpu.VMEM((n_fs, wr, n_w * ch), BF), pltpu.VMEM((n_fs, rows, n_tp * half), BF),
            pltpu.VMEM((n_sp * n_fs * wr, n_w * ch), BF), pltpu.VMEM((n_fs, rows, n_w * ch), F32),
            dma(2, 2), dma(n_fs, 2), dma(2), dma(n_fs, 2), dma(n_fs, 2), dma(n_fs - 1), dma(n_sp, n_fs),
            dma(n_sp, n_fs), dma(n_sp, n_fs), dma(n_fs - 1), dma(n_fs),
        ],
        1, "project",
    )(
        tokens[0], w_query, forget_weight, w_input, w_outgate, w_pool, extra, norm_gain[None],
        group_weight, pool_gain[None], recurrent_output_weight, w_out_pool,
    )
    n_half = n_sp // n_tp
    act, sq = comm(
        functools.partial(state_kernel, n_sp, group_weight.shape[1]),
        [((2, n_fs * rows, ch), BF), ((n_fs, 8, 128), F32)],
        [
            pltpu.VMEM((n_fs, rows, ch), F32), pltpu.VMEM((n_fs, rows, ch), F32),
            pltpu.VMEM((n_fs, ch, ch), BF), pltpu.VMEM((n_fs, 8, ch), F32),
            pltpu.VMEM((n_sp - 1, n_fs, ch, ch), BF), pltpu.VMEM((n_sp - 1, n_fs, 8, ch), F32),
            pltpu.VMEM((n_fs, 2**POOL_GROUPS, ch), BF),
            dma(n_sp - 1), dma(n_sp - 1), dma(n_sp - 1), dma(n_sp - 1), dma(), dma(),
        ],
        2, "state",
    )(z, e_all, forget_gap[None], rec_gain[None])
    out_shape = (n_fs, n_tp, rows // n_tp, n_half * cw)
    (final,) = comm(
        functools.partial(mix_kernel, n_sp, n_fs, n_tp),
        [((rows // n_tp, n_tp * n_half * n_fs * cw), BF)],
        [
            pltpu.VMEM(out_shape, BF), pltpu.VMEM((n_tp, n_fs) + act.shape, BF), pltpu.VMEM((n_tp, n_fs) + sq.shape, F32),
            pltpu.VMEM((n_half, n_tp) + ow.shape, BF), pltpu.VMEM((n_sp,) + ow.shape, BF),
            pltpu.VMEM((2, n_tp * width, n_half * cw), BF), pltpu.VMEM(out_shape, BF),
            dma(2, 2), dma(n_fs, 2), dma(2), dma(n_fs, 2), dma(n_fs, 2), dma(n_fs, n_tp), dma(n_tp, n_fs),
            dma(n_sp), dma(n_sp), dma(n_sp), dma(n_sp), dma(n_sp), dma(n_fs, n_tp), dma(n_fs, n_tp),
        ],
        3, "mix",
    )(act, sq, ow)
    return final[None]


def solution(mesh):
    sizes = dict(mesh.shape)
    weight = P(("sp", "fs"), "tp")
    placed = (
        P("fs", "sp", "tp"), P(), weight, weight, weight, weight, weight, P("tp"),
        P("fs", "sp", "tp"), P("tp"), P(), P("tp"), P("tp", ("sp", "fs")), P("tp", ("sp", "fs")),
    )
    return jax.shard_map(
        functools.partial(body, sizes["sp"], sizes["fs"], sizes["tp"]),
        mesh=mesh, in_specs=placed, out_specs=P("fs", ("sp", "tp"), None), check_vma=False,
    )
```
